32 devices in a mesh: grp: 2 (over y), sp: 4 (over z), tp: 4 (over x, core).
Axes of the slice: x: 2, y: 2, z: 4, core: 2. Of those that a mesh axis runs over, the one named last changes fastest.
Arguments:
- residual: bfloat16 [2048, 2048], P(('grp', 'sp')), parts along dimension 0, may hold values from -34 to 34
- queries: bfloat16 [2048, 1024], P(('grp', 'sp'), 'tp'), parts along dimension 0, may hold values from -400 to 400
- keys: bfloat16 [2048, 512], P(('grp', 'sp'), 'tp'), parts along dimension 0, may hold values from -8 to 8
- values: bfloat16 [2048, 512], P(('grp', 'sp'), 'tp'), parts along dimension 0, may hold values from -6 to 6
- segments: int32 [2048], P(('grp', 'sp')), parts along dimension 0, may hold values from 0 to 2, never falling along the last dimension, each value on 1 to 768 neighbouring positions
- routes: int32 [2048, 2], P(('grp', 'sp')), parts along dimension 0, may hold values from 0 to 3, all different within a row; in each aligned block of 256 rows (0 to 255, 256 to 511, ...) at most 256 rows name the same one
- route_weight: float32 [2048, 2], P(('grp', 'sp')), parts along dimension 0, may hold values from 0.3 to 3
- sinks: float32 [16], P('tp'), may hold values from 1 to 6
- out_weight: bfloat16 [1024, 2048], P('tp'), may hold values from -1 to 1
- norm_gain: float32 [2048], replicated, may hold values from 0.1 to 1.9
- expert_gate: bfloat16 [4, 2048, 1024], P('sp', None, 'tp'), may hold values from -0.125 to 0.125
- expert_up: bfloat16 [4, 2048, 1024], P('sp', None, 'tp'), may hold values from -0.125 to 0.125
- expert_down: bfloat16 [4, 1024, 2048], P('sp', None, 'tp'), may hold values from -0.1875 to 0.1875
- shared_gate: bfloat16 [2048, 1024], P(None, 'tp'), may hold values from -0.125 to 0.125
- shared_up: bfloat16 [2048, 1024], P(None, 'tp'), may hold values from -0.125 to 0.125
- shared_down: bfloat16 [1024, 2048], P(None, 'tp'), may hold values from -0.1875 to 0.1875
Outputs:
- mixed: bfloat16 [2048, 2048], P(('grp', 'sp'), 'tp'), parts along dimension 0
The draws below stay inside these ranges and needn't reach their ends.
There are 2 independent parts, one for each index of `grp`. The reference program is written for one: setup_inputs(seed, part) draws one part's arguments, and reference() takes and returns one part's arrays. A program takes and returns all parts, laid end to end along the dimension named above; an argument that names none is the same for every part. Nothing has to cross between parts.
Inputs may be any that keep to these rules, and one draw needn't show every extreme that they name: `routes`: each row names 2 different experts. In the rows of one device no expert is named by more than 256 rows, and in some device's rows an expert is named by exactly 256. `segments`: document numbers never fall along the positions; every document spans 1 to 768 positions and one spans exactly 768.
All inputs are finite; a program needn't handle non-finite values.
Results may differ from the reference program's by a relative error of at most 0.0065.
Values may be sent and summed in bfloat16 or wider, within the bound.
A program may use at most 64 MiB of HBM per device.

```python
import math
import jax
import jax.numpy as jnp
import numpy as np
from jax import lax

D = 2048
HEADS = 16
KV_HEADS = 8
HEAD_DIM = 64
WINDOW = 128
EFF = 1024
SFF = 1024
TOPK = 2
TOK = 256
TOKENS = 1024
EXPERTS = 4
CAP = 256
DOCS = 3
LONGEST = 768
N_SP = 4


def query_key_pair(key):
    query_seed = jax.random.fold_in(key, 101)
    key_seed = jax.random.fold_in(key, 202)
    queries = jnp.clip(jax.random.normal(query_seed, (TOKENS, HEADS * HEAD_DIM), jnp.float32), -6.0, 6.0)
    key_rows = jnp.clip(jax.random.normal(key_seed, (TOKENS, KV_HEADS * HEAD_DIM), jnp.float32), -6.0, 6.0)
    return (queries, key_rows)


def draw_queries(key, part):
    queries, key_rows = query_key_pair(key)
    return queries.astype(jnp.bfloat16)


def draw_keys(key, part):
    queries, key_rows = query_key_pair(key)
    return key_rows.astype(jnp.bfloat16)


def draw_residual(key, part):
    profile = jnp.exp(math.log(4.0) * jnp.arange(D, dtype=jnp.float32) / D)
    jitter = jnp.exp(jax.random.uniform(jax.random.fold_in(key, 11), (D,), jnp.float32, math.log(0.7), math.log(1.4)))
    base = jnp.clip(jax.random.normal(jax.random.fold_in(key, 14), (TOKENS, D), jnp.float32), -6.0, 6.0)
    return (base * profile * jitter).astype(jnp.bfloat16)


def level_of(own_key, shape, pieces, low, high):
    def one(dim, parts):
        heights = jax.random.uniform(jax.random.fold_in(jax.random.fold_in(own_key, 6), dim), (parts,), jnp.float32, low / len(pieces), high / len(pieces))
        return jnp.repeat(jnp.exp(heights), shape[dim] // parts).reshape((-1,) + (1,) * (len(shape) - dim - 1))

    factor_of = one(*pieces[0])
    for cut in pieces[1:]:
        factor_of = factor_of * one(*cut)
    return factor_of


def length_profile(amount, total, limit, skew):
    portions = [(1 << 20) // math.isqrt(grade ** skew) + 1 for grade in range(2, amount + 1)]
    rest, counts = total - limit - (amount - 1), [1] * (amount - 1)
    while rest > 0:
        movable = [i for i in range(amount - 1) if counts[i] < limit]
        whole, left = sum([portions[i] for i in movable]), rest
        for i in movable:
            addition = min(limit - counts[i], max(1, left * portions[i] // whole), rest)
            counts[i] = counts[i] + addition
            rest = rest - addition
    return np.array([limit] + counts)


def ragged(stream_key, count, total, reach, slope):
    if count == 2:
        one = jax.random.randint(stream_key, (), max(1, total - reach), min(reach, total - 1) + 1)
        return jnp.stack([one, total - one])
    sizes = jnp.asarray(length_profile(count, total, reach, slope), jnp.int32)
    twos = (count - 1) // 2
    source_of, taker = sizes[1:1 + 2 * twos:2], sizes[2:2 + 2 * twos:2]
    room = jnp.minimum(source_of - 1, reach - taker)
    passed = jax.random.randint(jax.random.fold_in(stream_key, 1), (twos,), 0, 1 << 20) % (room + 1)
    sizes = sizes.at[1:1 + 2 * twos:2].set(source_of - passed).at[2:2 + 2 * twos:2].set(taker + passed)
    return sizes[jax.random.permutation(jax.random.fold_in(stream_key, 2), count)]


def deal_out(key, own, number, rows, count, top, reach, lean):
    order = jax.random.permutation(key, count)
    heavy_load, usual = shares(count, rows * top, reach, lean, True), shares(count, rows * top, reach, lean, False)
    places = jnp.arange(count)

    def named(tallies, turn):
        used = int((tallies > 0).sum())
        fixed = max(1, used // 4)
        shifted = fixed + (places - fixed + turn * (used - fixed)) % max(1, count - fixed)
        return jnp.zeros((count,), jnp.int32).at[order[jnp.where(places < fixed, places, shifted)]].set(jnp.asarray(tallies, jnp.int32))

    tallies = jnp.where(number % 4 == 0, named(heavy_load, number // 4), named(usual, number - number // 4 - 1))
    mixed = jax.random.permutation(jax.random.fold_in(own, 3), count)
    source_of, taker = mixed[0:count // 2 * 2:2], mixed[1:count // 2 * 2:2]
    margin = jnp.minimum(tallies[source_of] - 1, reach - tallies[taker]) // 2
    margin = jnp.where((source_of == order[0]) | (taker == order[0]) | (tallies[taker] == 0), 0, jnp.maximum(margin, 0))
    shifted = jax.random.randint(jax.random.fold_in(own, 4), (count // 2,), 0, 1 << 20) % (margin + 1)
    tallies = tallies.at[source_of].add(-shifted).at[taker].add(shifted)
    members = jnp.searchsorted(jnp.cumsum(tallies), jnp.arange(rows * top), side="right").astype(jnp.int32)
    listing = members.reshape(top, rows).T
    listing = listing[jax.random.permutation(jax.random.fold_in(own, 1), rows)]
    turn = jax.random.randint(jax.random.fold_in(own, 2), (rows, 1), 0, top)
    return jnp.take_along_axis(listing, (jnp.arange(top)[None, :] + turn) % top, axis=1)


def shares(number_of, total, limit, skew, full):
    loads = [(1 << 20) // math.isqrt(grade ** skew) + 1 for grade in range(1, number_of + 1)]
    largest = limit if full else min(limit, max(-(-total // number_of), total * loads[0] // sum(loads)))
    least = 1 if total - largest >= number_of - 1 else 0
    counts, surplus = [largest] + [least] * (number_of - 1), total - largest - least * (number_of - 1)
    while surplus > 0:
        free = [i for i in range(1, number_of) if counts[i] < largest] or [i for i in range(1, number_of) if counts[i] < limit]
        mass, remaining = sum([loads[i] for i in free]), surplus
        for i in free:
            more = min(limit - counts[i], max(1, remaining * loads[i] // mass), surplus)
            counts[i] = counts[i] + more
            surplus = surplus - more
    return np.array(counts)


def centred(rng, extent, deviation, most, pieces=(), kind=jnp.bfloat16):
    array = jax.random.normal(rng, extent, jnp.float32) * deviation
    if len(pieces) > 0:
        array = level_of(rng, extent, pieces, -0.22, 0.18) * array
    return jnp.clip(array, min=-most, max=most).astype(kind)


def setup_inputs(seed: int = 0, part: int = 0) -> dict:
    key_of = jax.random.split(jax.random.key(seed), 17)
    part_keys = jax.random.split(jax.random.fold_in(key_of[16], part), 17)
    residual = draw_residual(jax.random.fold_in(jax.random.fold_in(key_of[16], part), 71), part)
    queries = draw_queries(jax.random.fold_in(jax.random.fold_in(key_of[16], part), 71), part)
    keys = draw_keys(jax.random.fold_in(jax.random.fold_in(key_of[16], part), 71), part)
    values = centred(part_keys[3], (TOKENS, KV_HEADS * HEAD_DIM), 1.0, 6.0, ((0, 4), (1, 4)))
    segments = jnp.searchsorted(jnp.cumsum(ragged(part_keys[4], DOCS, TOKENS, LONGEST, 2)), jnp.arange(TOKENS), side="right").astype(jnp.int32)
    routes_keys = jax.random.split(jax.random.fold_in(part_keys[5], 1), TOKENS // TOK)
    routes_turns = jax.random.permutation(jax.random.fold_in(part_keys[5], 3), TOKENS // TOK)
    routes = jax.vmap(lambda own, number: deal_out(jax.random.fold_in(part_keys[5], 2), own, number, TOK, EXPERTS, TOPK, CAP, 1))(routes_keys, routes_turns).reshape((TOKENS, TOPK))
    route_weight = jnp.clip(jnp.exp(math.log(3.0) - 2.3025851 * jax.random.uniform(part_keys[6], (TOKENS, TOPK), jnp.float32) ** level_of(part_keys[6], (TOKENS, TOPK), ((0, 4),), -0.2, 0.2)), 0.3, 3.0)
    sinks = jnp.clip(1.0 + 5.0 * jax.random.uniform(key_of[7], (HEADS,), jnp.float32) ** level_of(key_of[7], (HEADS,), ((0, 4),), -0.2, 0.2), 1.0, 6.0)
    out_weight = centred(key_of[8], (HEADS * HEAD_DIM, D), (HEADS * HEAD_DIM // 32) ** -0.5, 1.0, ((0, 4),))
    norm_gain = jnp.clip(1.0 + 0.18 * jax.random.normal(key_of[9], (D,), jnp.float32), 0.1, 1.9)
    expert_gate = centred(key_of[10], (EXPERTS, D, EFF), D ** -0.5, 0.125, ((0, 4), (2, 4)))
    expert_up = centred(key_of[11], (EXPERTS, D, EFF), D ** -0.5, 0.125, ((0, 4), (2, 4)))
    expert_down = centred(key_of[12], (EXPERTS, EFF, D), EFF ** -0.5, 0.1875, ((0, 4), (2, 4)))
    shared_gate = centred(key_of[13], (D, SFF), D ** -0.5, 0.125, ((1, 4),))
    shared_up = centred(key_of[14], (D, SFF), D ** -0.5, 0.125, ((1, 4),))
    shared_down = centred(key_of[15], (SFF, D), SFF ** -0.5, 0.1875, ((1, 4),))
    return {"residual": residual, "queries": queries, "keys": keys, "values": values, "segments": segments, "routes": routes, "route_weight": route_weight, "sinks": sinks, "out_weight": out_weight, "norm_gain": norm_gain, "expert_gate": expert_gate, "expert_up": expert_up, "expert_down": expert_down, "shared_gate": shared_gate, "shared_up": shared_up, "shared_down": shared_down}


epsilon = 1e-06

def banded(rows, fill):
    blocks = rows.shape[0] // WINDOW
    shaped = rows.reshape((blocks, WINDOW) + rows.shape[1:])
    before = jnp.concatenate([jnp.full_like(shaped[:1], fill), shaped[:-1]], axis=0)
    return jnp.concatenate([before, shaped], axis=1)

def attend(queries, keys, values, segments, sinks):
    blocks = TOKENS // WINDOW
    group_size = HEADS // KV_HEADS
    query_blocks = queries.astype(jnp.float32).reshape(blocks, WINDOW, KV_HEADS, group_size, HEAD_DIM)
    key_band = banded(keys, 0).astype(jnp.float32).reshape(blocks, 2 * WINDOW, KV_HEADS, HEAD_DIM)
    value_band = banded(values, 0).astype(jnp.float32).reshape(blocks, 2 * WINDOW, KV_HEADS, HEAD_DIM)
    segment_band = banded(segments, -1)
    query_segments = segments.reshape(blocks, WINDOW)
    scores = jnp.einsum('nqhgd,nkhd->nhgqk', query_blocks, key_band) * HEAD_DIM ** (-0.5)
    offsets = jnp.arange(WINDOW)[:, None] + WINDOW - jnp.arange(2 * WINDOW)[None, :]
    allowed = (offsets >= 0) & (offsets < WINDOW) & (query_segments[:, :, None] == segment_band[:, None, :])
    sink_logits = sinks.astype(jnp.float32).reshape(KV_HEADS, group_size)[None, :, :, None]
    masked = jnp.where(allowed[:, None, None], scores, -jnp.inf)
    top_score = jnp.maximum(lax.optimization_barrier(jnp.max(masked, axis=-1)), sink_logits)
    exp_terms = jnp.where(allowed[:, None, None], jnp.exp(scores - top_score[..., None]), 0.0)
    denominator = lax.optimization_barrier(jnp.sum(exp_terms, axis=-1)) + jnp.exp(sink_logits - top_score)
    probabilities = (exp_terms / denominator[..., None]).astype(jnp.bfloat16)
    attended = jnp.einsum('nhgqk,nkhd->nqhgd', probabilities.astype(jnp.float32), value_band)
    return attended.astype(jnp.bfloat16).reshape(TOKENS, HEADS * HEAD_DIM)

def block_slots(block_routes):
    flat_ids = block_routes.reshape(-1)
    one_hot = (flat_ids[:, None] == jnp.arange(EXPERTS, dtype=jnp.int32)[None, :]).astype(jnp.int32)
    rank_in = jnp.cumsum(one_hot, axis=0) - one_hot
    return flat_ids * CAP + lax.optimization_barrier(jnp.sum(rank_in * one_hot, axis=1))

def reference(residual, queries, keys, values, segments, routes, route_weight, sinks, out_weight, norm_gain, expert_gate, expert_up, expert_down, shared_gate, shared_up, shared_down):
    attended = attend(queries, keys, values, segments, sinks)
    projected = jnp.dot(attended, out_weight, preferred_element_type=jnp.float32)
    updated = (residual.astype(jnp.float32) + projected).astype(jnp.bfloat16)
    updated_f32 = updated.astype(jnp.float32)
    inv_rms = lax.rsqrt(lax.optimization_barrier(jnp.mean(updated_f32 * updated_f32, axis=-1, keepdims=True)) + epsilon)
    normed = (updated_f32 * inv_rms * norm_gain).astype(jnp.bfloat16)
    shared_pre = jnp.dot(normed, shared_gate, preferred_element_type=jnp.float32)
    shared_lin = jnp.dot(normed, shared_up, preferred_element_type=jnp.float32)
    shared_act = (jax.nn.silu(shared_pre) * shared_lin).astype(jnp.bfloat16)
    shared_out = jnp.dot(shared_act, shared_down, preferred_element_type=jnp.float32)
    slot_dest = jax.vmap(block_slots)(routes.reshape(N_SP, TOK, TOPK))
    block_ids = jnp.broadcast_to(jnp.arange(N_SP, dtype=jnp.int32)[:, None], slot_dest.shape)
    token_ids = block_ids * TOK + (jnp.arange(TOK * TOPK, dtype=jnp.int32) // TOPK)[None, :]
    slot_token = jnp.full((N_SP, EXPERTS * CAP), -1, jnp.int32).at[block_ids, slot_dest].set(token_ids)
    slot_weight = jnp.zeros((N_SP, EXPERTS * CAP), jnp.float32).at[block_ids, slot_dest].set(route_weight.reshape(N_SP, TOK * TOPK))
    per_token = slot_token.reshape(N_SP, EXPERTS, CAP).transpose(1, 0, 2).reshape(EXPERTS, N_SP * CAP)
    per_weight = slot_weight.reshape(N_SP, EXPERTS, CAP).transpose(1, 0, 2).reshape(EXPERTS, N_SP * CAP)

    def one_expert(accum, inputs):
        gate_mat, up_mat, down_mat, token_list, weight_list = inputs
        filled = token_list >= 0
        safe_token = jnp.where(filled, token_list, 0).astype(jnp.int32)
        rows_in = jnp.where(filled[:, None], normed[safe_token], jnp.zeros((), jnp.bfloat16))
        gate_pre = jnp.dot(rows_in, gate_mat, preferred_element_type=jnp.float32)
        up_lin = jnp.dot(rows_in, up_mat, preferred_element_type=jnp.float32)
        expert_act = (jax.nn.silu(gate_pre) * up_lin).astype(jnp.bfloat16)
        expert_out = jnp.dot(expert_act, down_mat, preferred_element_type=jnp.float32).astype(jnp.bfloat16)
        accum = accum.at[safe_token].add(expert_out.astype(jnp.float32) * weight_list[:, None])
        return (accum, None)
    routed, _ = lax.scan(one_expert, jnp.zeros((TOKENS, D), jnp.float32), (expert_gate, expert_up, expert_down, per_token, per_weight))
    return (updated_f32 + shared_out + routed).astype(jnp.bfloat16)
```

```python
import functools
import jax
import jax.numpy as jnp
from jax import lax
from jax.experimental import pallas as pl
from jax.experimental.pallas import tpu as pltpu
from jax.sharding import PartitionSpec as P

HEAD_DIM = 64
WINDOW = 128


epsilon = 1e-06


def passed_along(value, axis, steps):
    count = lax.axis_size(axis)
    leading, last = (max(0, -steps), min(count, count - steps))
    return lax.ppermute(value, axis, [(source, source + steps) for source in range(leading, last)])


def banded(prev_rows, own_rows, window_len):
    blocks = own_rows.shape[0] // window_len
    joined = jnp.concatenate([prev_rows, own_rows], axis=0)
    shaped = joined.reshape((blocks + 1, window_len) + own_rows.shape[1:])
    return jnp.concatenate([shaped[:-1], shaped[1:]], axis=1)


def shards(
    residual,
    queries,
    keys,
    values,
    segments,
    routes,
    route_weight,
    sinks,
    out_weight,
    norm_gain,
    expert_gate,
    expert_up,
    expert_down,
    shared_gate,
    shared_up,
    shared_down,
):
    rows_here = residual.shape[0]
    model_width = residual.shape[1]
    tp_count = lax.axis_size("tp")
    tp_index = lax.axis_index("tp")
    head_local = queries.shape[1] // HEAD_DIM
    kv_local = keys.shape[1] // HEAD_DIM
    group_size = head_local // kv_local
    window_len = WINDOW
    blocks = rows_here // window_len
    own_marks = (segments % 256 + 1).astype(jnp.bfloat16)
    prev_keys, prev_values, prev_marks = passed_along(
        (
            keys[rows_here - window_len :],
            values[rows_here - window_len :],
            own_marks[rows_here - window_len :],
        ),
        "sp",
        1,
    )
    key_band = banded(prev_keys, keys, window_len).reshape(
        blocks, 2 * window_len, kv_local, HEAD_DIM
    )
    value_band = banded(prev_values, values, window_len).reshape(
        blocks, 2 * window_len, kv_local, HEAD_DIM
    )
    mark_band = banded(prev_marks, own_marks, window_len).astype(jnp.float32)
    query_marks = own_marks.reshape(blocks, window_len).astype(jnp.float32)
    query_blocks = queries.reshape(blocks, window_len, kv_local, group_size, HEAD_DIM)
    scores = jnp.einsum(
        "nqhgd,nkhd->nhgqk", query_blocks, key_band, preferred_element_type=jnp.float32
    ) * HEAD_DIM ** (-0.5)
    offsets = jnp.arange(window_len)[:, None] + window_len - jnp.arange(2 * window_len)[None, :]
    allowed = (
        (offsets >= 0) & (offsets < window_len) & (query_marks[:, :, None] == mark_band[:, None, :])
    )
    sink_logits = sinks.reshape(kv_local, group_size)[None, :, :, None]
    masked = jnp.where(allowed[:, None, None], scores, -jnp.inf)
    top_score = jnp.maximum(jnp.max(masked, axis=-1), sink_logits)
    exp_terms = jnp.where(allowed[:, None, None], jnp.exp(scores - top_score[..., None]), 0.0)
    denominator = jnp.sum(exp_terms, axis=-1) + jnp.exp(sink_logits - top_score)
    probabilities = (exp_terms / denominator[..., None]).astype(jnp.bfloat16)
    attended = jnp.einsum(
        "nhgqk,nkhd->nqhgd", probabilities, value_band, preferred_element_type=jnp.float32
    )
    attended = attended.astype(jnp.bfloat16).reshape(rows_here, head_local * HEAD_DIM)
    partial_value = jnp.dot(attended, out_weight, preferred_element_type=jnp.float32)
    col_width = model_width // tp_count
    col_start = tp_index * col_width
    summed = lax.psum(partial_value, "tp")
    updated = (residual.astype(jnp.float32) + summed).astype(jnp.bfloat16)
    updated_f32 = updated.astype(jnp.float32)
    inv_rms = lax.rsqrt(jnp.mean(updated_f32 * updated_f32, axis=-1, keepdims=True) + epsilon)
    normed = (updated_f32 * inv_rms * norm_gain).astype(jnp.bfloat16)
    updated_cols = lax.dynamic_slice_in_dim(updated, col_start, col_width, 1)
    normed_cols = lax.dynamic_slice_in_dim(normed, col_start, col_width, 1)
    shared_pre = jnp.dot(normed, shared_gate, preferred_element_type=jnp.float32)
    shared_lin = jnp.dot(normed, shared_up, preferred_element_type=jnp.float32)
    shared_act = (jax.nn.silu(shared_pre) * shared_lin).astype(jnp.bfloat16)
    top_count = routes.shape[1]
    experts = lax.axis_size("sp")
    capacity = 2 * rows_here * top_count // experts
    flat_ids = routes.reshape(-1)
    one_hot = (flat_ids[:, None] == jnp.arange(experts, dtype=jnp.int32)[None, :]).astype(jnp.int32)
    rank_in = jnp.cumsum(one_hot, axis=0) - one_hot
    slot_dest = flat_ids * capacity + jnp.sum(rank_in * one_hot, axis=1)
    token_of = jnp.arange(rows_here * top_count, dtype=jnp.int32) // top_count
    slot_token = jnp.full((experts * capacity,), -1, jnp.int32).at[slot_dest].set(token_of)
    filled = slot_token >= 0
    safe_token = jnp.where(filled, slot_token, 0)
    outgoing = jnp.where(filled[:, None], normed_cols[safe_token], jnp.zeros((), jnp.bfloat16))
    pieces = lax.all_to_all(
        outgoing.reshape(experts, capacity, col_width),
        "sp",
        split_axis=0,
        concat_axis=0,
        tiled=True,
    )
    arrived = lax.all_gather(pieces, "tp", axis=2, tiled=True)
    expert_rows = arrived.reshape(-1, model_width)
    gate_pre = jnp.dot(expert_rows, expert_gate[0], preferred_element_type=jnp.float32)
    up_lin = jnp.dot(expert_rows, expert_up[0], preferred_element_type=jnp.float32)
    expert_act = (jax.nn.silu(gate_pre) * up_lin).astype(jnp.bfloat16)
    gathered_expert, gathered_shared = (
        lax.all_gather(expert_act, "tp", axis=1, tiled=True),
        lax.all_gather(shared_act, "tp", axis=1, tiled=True),
    )
    expert_out = jnp.dot(
        gathered_expert, expert_down[0], preferred_element_type=jnp.float32
    ).astype(jnp.bfloat16)
    returned = lax.all_to_all(
        expert_out.reshape(experts, capacity, col_width),
        "sp",
        split_axis=0,
        concat_axis=0,
        tiled=True,
    )
    returned = returned.reshape(experts * capacity, col_width)
    picked = returned[slot_dest].astype(jnp.float32).reshape(rows_here, top_count, col_width)
    routed = jnp.sum(picked * route_weight[:, :, None], axis=1)
    shared_cols = jnp.dot(gathered_shared, shared_down, preferred_element_type=jnp.float32)
    return (updated_cols.astype(jnp.float32) + shared_cols + routed).astype(jnp.bfloat16)


MESH = pl.DeviceIdType.MESH


def fused_kernel(
    dims,
    res_hbm,
    q_ref,
    k_ref,
    v_ref,
    seg_row,
    seg_col,
    routes_ref,
    rw_ref,
    sinks_ref,
    wo_hbm,
    gain_ref,
    eg_hbm,
    eu_hbm,
    ed_hbm,
    sg_hbm,
    su_hbm,
    sd_hbm,
    out_ref,
    res_v,
    wo_v,
    gu_v,
    sgu_v,
    dn_v,
    sdn_v,
    kh,
    vh,
    mh,
    att,
    b1s,
    b1r,
    b2s,
    b2r,
    keep,
    upd,
    norm_v,
    act,
    eout,
    eback,
    acc,
    w_sem,
    halo_s,
    halo_r,
    b_s,
    b_r,
    u_s,
    u_r,
    a_s,
    a_r,
    e_s,
    e_r,
):
    rows, cols, width, window, hidden, heads, group = dims
    bf16, f32 = jnp.bfloat16, jnp.float32
    s = lax.axis_index("sp")
    t = lax.axis_index("tp")
    core = t % 2
    chip = t // 2
    mate = t + 1 - 2 * core
    over = t + 2 - 4 * chip
    diag = 3 - t

    def remote(src, dst, send, recv, sp, tp):
        return pltpu.make_async_remote_copy(
            src_ref=src,
            dst_ref=dst,
            send_sem=send,
            recv_sem=recv,
            device_id={"sp": sp, "tp": tp},
            device_id_type=MESH,
        )

    own_cols = pl.ds(pl.multiple_of(t * cols, cols), cols)
    loads = [
        pltpu.make_async_copy(wo_hbm, wo_v, w_sem.at[0]),
        pltpu.make_async_copy(res_hbm.at[:, own_cols], res_v, w_sem.at[1]),
        pltpu.make_async_copy(eg_hbm.at[0], gu_v.at[:, pl.ds(0, hidden)], w_sem.at[2]),
        pltpu.make_async_copy(eu_hbm.at[0], gu_v.at[:, pl.ds(hidden, hidden)], w_sem.at[3]),
        pltpu.make_async_copy(sg_hbm, sgu_v.at[:, pl.ds(0, hidden)], w_sem.at[4]),
        pltpu.make_async_copy(su_hbm, sgu_v.at[:, pl.ds(hidden, hidden)], w_sem.at[5]),
        pltpu.make_async_copy(ed_hbm.at[0], dn_v, w_sem.at[6]),
        pltpu.make_async_copy(sd_hbm, sdn_v, w_sem.at[7]),
    ]
    for load in loads:
        load.start()

    barrier = pltpu.get_barrier_semaphore()
    pl.semaphore_signal(barrier, inc=1, device_id={"sp": s, "tp": mate}, device_id_type=MESH)
    pl.semaphore_signal(barrier, inc=1, device_id={"sp": s, "tp": over}, device_id_type=MESH)
    for step in range(1, 4):
        pl.semaphore_signal(
            barrier, inc=1, device_id={"sp": (s + step) % 4, "tp": t}, device_id_type=MESH
        )
    pl.semaphore_wait(barrier, 5)

    tail = pl.ds(rows - window, window)
    up_sp, down_sp = (s + 1) % 4, (s + 3) % 4
    halos = [
        remote(k_ref.at[tail], kh, halo_s.at[0], halo_r.at[0], up_sp, t),
        remote(v_ref.at[tail], vh, halo_s.at[1], halo_r.at[1], up_sp, t),
        remote(seg_row.at[:, tail], mh, halo_s.at[2], halo_r.at[2], up_sp, t),
    ]

    @pl.when(s < 3)
    def _():
        for copy in halos:
            copy.start()

    @pl.when(s == 0)
    def _():
        kh[...] = jnp.zeros_like(kh)
        vh[...] = jnp.zeros_like(vh)
        mh[...] = jnp.full(mh.shape, -1.0, f32)

    q_pos = lax.broadcasted_iota(jnp.int32, (window, window), 0)
    k_pos = lax.broadcasted_iota(jnp.int32, (window, window), 1)

    def attend(n):
        here = pl.ds(n * window, window)
        if n == 0:
            k_prev, v_prev, m_prev = kh[...], vh[...], mh[0:1, :]
        else:
            before = pl.ds((n - 1) * window, window)
            k_prev, v_prev, m_prev = k_ref[before, :], v_ref[before, :], seg_row[0:1, before]
        k_own, v_own, m_own = k_ref[here, :], v_ref[here, :], seg_row[0:1, here]
        marks = seg_col[here, :]
        ok_prev = (k_pos > q_pos) & (marks == m_prev)
        ok_own = (k_pos <= q_pos) & (marks == m_own)
        for h in range(heads):
            kv = slice((h // group) * HEAD_DIM, (h // group + 1) * HEAD_DIM)
            qh = q_ref[here, h * HEAD_DIM : (h + 1) * HEAD_DIM]
            contract = (((1,), (1,)), ((), ()))
            sc_prev = lax.dot_general(
                qh, k_prev[:, kv], contract, preferred_element_type=f32
            ) * HEAD_DIM ** (-0.5)
            sc_own = lax.dot_general(
                qh, k_own[:, kv], contract, preferred_element_type=f32
            ) * HEAD_DIM ** (-0.5)
            sc_prev = jnp.where(ok_prev, sc_prev, -jnp.inf)
            sc_own = jnp.where(ok_own, sc_own, -jnp.inf)
            sink = sinks_ref[h]
            top = jnp.maximum(
                jnp.max(jnp.maximum(sc_prev, sc_own), axis=-1, keepdims=True), sink
            )
            ex_prev = jnp.exp(sc_prev - top)
            ex_own = jnp.exp(sc_own - top)
            total = jnp.sum(ex_prev + ex_own, axis=-1, keepdims=True) + jnp.exp(sink - top)
            p_prev = (ex_prev / total).astype(bf16)
            p_own = (ex_own / total).astype(bf16)
            got = jnp.dot(p_prev, v_prev[:, kv], preferred_element_type=f32) + jnp.dot(
                p_own, v_own[:, kv], preferred_element_type=f32
            )
            att[here, h * HEAD_DIM : (h + 1) * HEAD_DIM] = got.astype(bf16)

    def project(n, chunk):
        where = pl.ds(pl.multiple_of(chunk * cols, cols), cols)
        return jnp.dot(
            att[pl.ds(n * window, window), :], wo_v[:, where], preferred_element_type=f32
        )

    halves = list(range(rows // window))[::-1]
    pending = []
    first = {}
    for n in halves:
        if n == 0:

            @pl.when(s > 0)
            def _():
                for copy in halos:
                    copy.wait_recv()

        attend(n)
        if n == halves[0]:
            loads[0].wait()
        for far in (1, 0):
            chunk = (over if far else t) + 1 - 2 * core
            b1s[n, far] = project(n, chunk).astype(bf16)
            copy = remote(
                b1s.at[n, far], b1r.at[n, far], b_s.at[n, far], b_r.at[n, far], s, mate
            )
            copy.start()
            pending.append(copy)
            first[n, far] = copy
    second = {}
    for n in halves:
        mine = project(n, over)
        first[n, 1].wait_recv()
        b2s[n] = (mine + b1r[n, 1].astype(f32)).astype(bf16)
        copy = remote(b2s.at[n], b2r.at[n], b_s.at[n, 2], b_r.at[n, 2], s, over)
        copy.start()
        pending.append(copy)
        second[n] = copy
    loads[1].wait()
    for n in halves:
        here = pl.ds(n * window, window)
        mine = project(n, t) + res_v[here, :].astype(f32)
        first[n, 0].wait_recv()
        keep[here, :] = mine + b1r[n, 0].astype(f32)

    def piece(b, chunk, n):
        return upd.at[b, chunk, pl.ds(n * window, window)]

    def share(kind, k, b, chunk, n, sp, tp):
        return remote(
            piece(b, chunk, n),
            piece(b, chunk, n),
            u_s.at[kind, k, n],
            u_r.at[b, chunk, n],
            sp,
            tp,
        )

    conditional = []
    for n in halves:
        here = pl.ds(n * window, window)
        second[n].wait_recv()
        upd[s, t, here, :] = (keep[here, :] + b2r[n].astype(f32)).astype(bf16)
        over_copy = share(3, 0, s, t, n, s, over)
        over_copy.start()
        up_copy = share(0, 0, s, t, n, up_sp, t)
        down_copy = share(1, 0, s, t, n, down_sp, t)

        @pl.when(s < 3)
        def _():
            up_copy.start()

        @pl.when(s > 0)
        def _():
            down_copy.start()

        mate_copy = share(2, 0, s, t, n, s, mate)
        mate_copy.start()
        pending += [over_copy, mate_copy]
        conditional += [(s < 3, up_copy), (s > 0, down_copy)]

    side = s // 2
    edge = s + side * (3 - 2 * s)
    order = [s]
    for k in range(1, 4):
        flat = k - edge if k == 1 else k
        order.append(flat + side * (3 - 2 * flat))

    def arrive(k):
        b = order[k]
        for n in halves:
            share(0, k, b, t, n, s, mate).wait_recv()
            copy = share(3, k, b, t, n, s, over)
            copy.start()
            to_up = share(0, k, b, t, n, up_sp, t)
            to_down = share(1, k, b, t, n, down_sp, t)
            rising = (b < s) & (s < 3)
            falling = (b > s) & (s > 0)

            @pl.when(rising)
            def _():
                to_up.start()

            @pl.when(falling)
            def _():
                to_down.start()

            conditional.extend([(rising, to_up), (falling, to_down)])
            mate_copy = share(2, k, b, t, n, s, mate)
            mate_copy.start()
            pending.extend([copy, mate_copy])

    def relay(k):
        b = order[k]
        for n in halves:
            share(4, k, b, over, n, s, mate).wait_recv()
            copy = share(4, k, b, over, n, s, mate)
            copy.start()
            pending.append(copy)

    def normalize(k):
        b = order[k]
        for n in halves:
            share(2, k, b, mate, n, s, mate).wait_recv()
            share(4, k, b, diag, n, s, mate).wait_recv()
        step = 32

        def body(i, carry):
            here = pl.ds(pl.multiple_of(i * step, step), step)
            squares = jnp.zeros((step, 1), f32)
            for chunk in range(4):
                part = upd[b, chunk, here, :].astype(f32)
                squares = squares + jnp.sum(part * part, axis=-1, keepdims=True)
            inv = lax.rsqrt(squares / width + epsilon)
            for chunk in range(4):
                part = upd[b, chunk, here, :].astype(f32)
                span = slice(chunk * cols, (chunk + 1) * cols)
                norm_v[here, span] = (part * inv * gain_ref[0:1, span]).astype(bf16)
            return carry

        lax.fori_loop(0, rows // step, body, 0)

    def pass_on(slot, kind, chunk, tp):
        return remote(
            act.at[slot, chunk],
            act.at[slot, chunk],
            a_s.at[kind, slot],
            a_r.at[slot, chunk],
            s,
            tp,
        )

    def activate(slot, weight):
        both = jnp.dot(norm_v[...], weight[...], preferred_element_type=f32)
        gate, lin = both[:, :hidden], both[:, hidden:]
        act[slot, t] = (gate / (1.0 + jnp.exp(-gate)) * lin).astype(bf16)
        for kind, tp in ((0, over), (1, mate)):
            copy = pass_on(slot, kind, t, tp)
            copy.start()
            pending.append(copy)

    def relay_act(slot):
        pass_on(slot, 2, over, mate).wait_recv()
        copy = pass_on(slot, 2, over, mate)
        copy.start()
        pending.append(copy)

    def contract_act(slot, weight):
        pass_on(slot, 1, mate, mate).wait_recv()
        pass_on(slot, 2, diag, mate).wait_recv()
        total = None
        for chunk in range(4):
            part = jnp.dot(
                act[slot, chunk],
                weight[chunk * hidden : (chunk + 1) * hidden, :],
                preferred_element_type=f32,
            )
            total = part if total is None else total + part
        return total


    def finish(k):
        eout[k] = contract_act(k, dn_v).astype(bf16)
        copy = remote(eout.at[k], eback.at[s], e_s.at[k], e_r.at[s], order[k], t)
        copy.start()
        pending.append(copy)

    relay(0)
    arrive(1)
    loads[2].wait()
    loads[3].wait()
    normalize(0)
    activate(0, gu_v)
    loads[4].wait()
    loads[5].wait()
    activate(4, sgu_v)
    relay(1)
    arrive(2)
    normalize(1)
    activate(1, gu_v)
    relay_act(0)
    relay_act(4)
    relay(2)
    arrive(3)
    normalize(2)
    activate(2, gu_v)
    relay_act(1)
    relay(3)
    loads[6].wait()
    finish(1)
    normalize(3)
    activate(3, gu_v)
    relay_act(2)
    finish(2)
    eout[0] = contract_act(0, dn_v).astype(bf16)
    loads[7].wait()
    acc[...] = contract_act(4, sdn_v)
    relay_act(3)
    finish(3)

    def weight_of(e):
        total = jnp.zeros((rows, 1), f32)
        for k in range(routes_ref.shape[1]):
            total = total + jnp.where(
                routes_ref[:, k : k + 1] == e, rw_ref[:, k : k + 1], 0.0
            )
        return total

    acc[...] = (
        acc[...]
        + upd[s, t].astype(f32)
        + weight_of(s) * eout[0].astype(f32)
    )
    for k in range(1, 4):
        b = order[k]
        remote(eout.at[k], eback.at[b], e_s.at[k], e_r.at[b], b, t).wait_recv()
        acc[...] = acc[...] + weight_of(b) * eback[b].astype(f32)
    out_ref[...] = acc[...].astype(bf16)

    for copy in pending:
        copy.wait_send()
    for when, copy in conditional:

        @pl.when(when)
        def _():
            copy.wait_send()

    @pl.when(s < 3)
    def _():
        for copy in halos:
            copy.wait_send()


def layer(
    residual,
    queries,
    keys,
    values,
    segments,
    routes,
    route_weight,
    sinks,
    out_weight,
    norm_gain,
    expert_gate,
    expert_up,
    expert_down,
    shared_gate,
    shared_up,
    shared_down,
):
    arguments = (
        residual,
        queries,
        keys,
        values,
        segments,
        routes,
        route_weight,
        sinks,
        out_weight,
        norm_gain,
        expert_gate,
        expert_up,
        expert_down,
        shared_gate,
        shared_up,
        shared_down,
    )
    rows, width = residual.shape
    n_sp, n_tp = lax.axis_size("sp"), lax.axis_size("tp")
    capacity = 2 * rows * routes.shape[1] // n_sp
    hidden = expert_gate.shape[2]
    if n_sp != 4 or n_tp != 4 or capacity < rows or shared_gate.shape[1] != hidden:
        return shards(*arguments)
    cols = width // n_tp
    heads = queries.shape[1] // HEAD_DIM
    group = queries.shape[1] // keys.shape[1]
    kv_width = keys.shape[1]
    blocks = rows // WINDOW
    bf16, f32 = jnp.bfloat16, jnp.float32
    marks = segments.astype(f32)
    vmem = pl.BlockSpec(memory_space=pltpu.VMEM)
    anywhere = pl.BlockSpec(memory_space=pl.ANY)
    dma = pltpu.SemaphoreType.DMA
    return pl.pallas_call(
        functools.partial(fused_kernel, (rows, cols, width, WINDOW, hidden, heads, group)),
        out_shape=jax.ShapeDtypeStruct((rows, cols), bf16),
        in_specs=[anywhere]
        + [vmem] * 7
        + [pl.BlockSpec(memory_space=pltpu.SMEM), anywhere, vmem]
        + [anywhere] * 6,
        out_specs=vmem,
        scratch_shapes=[
            pltpu.VMEM((rows, cols), bf16),
            pltpu.VMEM(out_weight.shape, bf16),
            pltpu.VMEM((width, 2 * hidden), bf16),
            pltpu.VMEM((width, 2 * hidden), bf16),
            pltpu.VMEM(expert_down.shape[1:], bf16),
            pltpu.VMEM(shared_down.shape, bf16),
            pltpu.VMEM((WINDOW, kv_width), bf16),
            pltpu.VMEM((WINDOW, kv_width), bf16),
            pltpu.VMEM((8, WINDOW), f32),
            pltpu.VMEM((rows, heads * HEAD_DIM), bf16),
            pltpu.VMEM((blocks, 2, WINDOW, cols), bf16),
            pltpu.VMEM((blocks, 2, WINDOW, cols), bf16),
            pltpu.VMEM((blocks, WINDOW, cols), bf16),
            pltpu.VMEM((blocks, WINDOW, cols), bf16),
            pltpu.VMEM((rows, cols), f32),
            pltpu.VMEM((4, 4, rows, cols), bf16),
            pltpu.VMEM((rows, width), bf16),
            pltpu.VMEM((5, 4, rows, hidden), bf16),
            pltpu.VMEM((4, rows, cols), bf16),
            pltpu.VMEM((4, rows, cols), bf16),
            pltpu.VMEM((rows, cols), f32),
            dma((8,)),
            dma((3,)),
            dma((3,)),
            dma((blocks, 3)),
            dma((blocks, 3)),
            dma((5, 4, blocks)),
            dma((4, 4, blocks)),
            dma((3, 5)),
            dma((5, 4)),
            dma((4,)),
            dma((4,)),
        ],
        compiler_params=pltpu.CompilerParams(collective_id=0, has_side_effects=True),
    )(
        residual,
        queries,
        keys,
        values,
        jnp.broadcast_to(marks[None, :], (8, rows)),
        marks[:, None],
        routes,
        route_weight,
        sinks,
        out_weight,
        norm_gain[None, :],
        expert_gate,
        expert_up,
        expert_down,
        shared_gate,
        shared_up,
        shared_down,
    )


def solution(mesh):
    placed = (
        P(("grp", "sp"), None),
        P(("grp", "sp"), "tp"),
        P(("grp", "sp"), "tp"),
        P(("grp", "sp"), "tp"),
        P(("grp", "sp")),
        P(("grp", "sp"), None),
        P(("grp", "sp"), None),
        P("tp"),
        P("tp", None),
        P(),
        P("sp", None, "tp"),
        P("sp", None, "tp"),
        P("sp", None, "tp"),
        P(None, "tp"),
        P(None, "tp"),
        P(None, "tp"),
    )
    return jax.shard_map(
        layer, mesh=mesh, in_specs=placed, out_specs=P(("grp", "sp"), "tp"), check_vma=False
    )
```

```python
import functools
import jax
import jax.numpy as jnp
from jax import lax
from jax.experimental import pallas as pl
from jax.experimental.pallas import tpu as pltpu
from jax.sharding import PartitionSpec as P

HEAD_DIM = 64
WINDOW = 128


epsilon = 1e-06


def passed_along(value, axis, steps):
    count = lax.axis_size(axis)
    leading, last = (max(0, -steps), min(count, count - steps))
    return lax.ppermute(value, axis, [(source, source + steps) for source in range(leading, last)])


def banded(prev_rows, own_rows, window_len):
    blocks = own_rows.shape[0] // window_len
    joined = jnp.concatenate([prev_rows, own_rows], axis=0)
    shaped = joined.reshape((blocks + 1, window_len) + own_rows.shape[1:])
    return jnp.concatenate([shaped[:-1], shaped[1:]], axis=1)


def shards(
    residual,
    queries,
    keys,
    values,
    segments,
    routes,
    route_weight,
    sinks,
    out_weight,
    norm_gain,
    expert_gate,
    expert_up,
    expert_down,
    shared_gate,
    shared_up,
    shared_down,
):
    rows_here = residual.shape[0]
    model_width = residual.shape[1]
    tp_count = lax.axis_size("tp")
    tp_index = lax.axis_index("tp")
    head_local = queries.shape[1] // HEAD_DIM
    kv_local = keys.shape[1] // HEAD_DIM
    group_size = head_local // kv_local
    window_len = WINDOW
    blocks = rows_here // window_len
    own_marks = (segments % 256 + 1).astype(jnp.bfloat16)
    prev_keys, prev_values, prev_marks = passed_along(
        (
            keys[rows_here - window_len :],
            values[rows_here - window_len :],
            own_marks[rows_here - window_len :],
        ),
        "sp",
        1,
    )
    key_band = banded(prev_keys, keys, window_len).reshape(
        blocks, 2 * window_len, kv_local, HEAD_DIM
    )
    value_band = banded(prev_values, values, window_len).reshape(
        blocks, 2 * window_len, kv_local, HEAD_DIM
    )
    mark_band = banded(prev_marks, own_marks, window_len).astype(jnp.float32)
    query_marks = own_marks.reshape(blocks, window_len).astype(jnp.float32)
    query_blocks = queries.reshape(blocks, window_len, kv_local, group_size, HEAD_DIM)
    scores = jnp.einsum(
        "nqhgd,nkhd->nhgqk", query_blocks, key_band, preferred_element_type=jnp.float32
    ) * HEAD_DIM ** (-0.5)
    offsets = jnp.arange(window_len)[:, None] + window_len - jnp.arange(2 * window_len)[None, :]
    allowed = (
        (offsets >= 0) & (offsets < window_len) & (query_marks[:, :, None] == mark_band[:, None, :])
    )
    sink_logits = sinks.reshape(kv_local, group_size)[None, :, :, None]
    masked = jnp.where(allowed[:, None, None], scores, -jnp.inf)
    top_score = jnp.maximum(jnp.max(masked, axis=-1), sink_logits)
    exp_terms = jnp.where(allowed[:, None, None], jnp.exp(scores - top_score[..., None]), 0.0)
    denominator = jnp.sum(exp_terms, axis=-1) + jnp.exp(sink_logits - top_score)
    probabilities = (exp_terms / denominator[..., None]).astype(jnp.bfloat16)
    attended = jnp.einsum(
        "nhgqk,nkhd->nqhgd", probabilities, value_band, preferred_element_type=jnp.float32
    )
    attended = attended.astype(jnp.bfloat16).reshape(rows_here, head_local * HEAD_DIM)
    partial_value = jnp.dot(attended, out_weight, preferred_element_type=jnp.float32)
    col_width = model_width // tp_count
    col_start = tp_index * col_width
    summed = lax.psum(partial_value, "tp")
    updated = (residual.astype(jnp.float32) + summed).astype(jnp.bfloat16)
    updated_f32 = updated.astype(jnp.float32)
    inv_rms = lax.rsqrt(jnp.mean(updated_f32 * updated_f32, axis=-1, keepdims=True) + epsilon)
    normed = (updated_f32 * inv_rms * norm_gain).astype(jnp.bfloat16)
    updated_cols = lax.dynamic_slice_in_dim(updated, col_start, col_width, 1)
    normed_cols = lax.dynamic_slice_in_dim(normed, col_start, col_width, 1)
    shared_pre = jnp.dot(normed, shared_gate, preferred_element_type=jnp.float32)
    shared_lin = jnp.dot(normed, shared_up, preferred_element_type=jnp.float32)
    shared_act = (jax.nn.silu(shared_pre) * shared_lin).astype(jnp.bfloat16)
    top_count = routes.shape[1]
    experts = lax.axis_size("sp")
    capacity = 2 * rows_here * top_count // experts
    flat_ids = routes.reshape(-1)
    one_hot = (flat_ids[:, None] == jnp.arange(experts, dtype=jnp.int32)[None, :]).astype(jnp.int32)
    rank_in = jnp.cumsum(one_hot, axis=0) - one_hot
    slot_dest = flat_ids * capacity + jnp.sum(rank_in * one_hot, axis=1)
    token_of = jnp.arange(rows_here * top_count, dtype=jnp.int32) // top_count
    slot_token = jnp.full((experts * capacity,), -1, jnp.int32).at[slot_dest].set(token_of)
    filled = slot_token >= 0
    safe_token = jnp.where(filled, slot_token, 0)
    outgoing = jnp.where(filled[:, None], normed_cols[safe_token], jnp.zeros((), jnp.bfloat16))
    pieces = lax.all_to_all(
        outgoing.reshape(experts, capacity, col_width),
        "sp",
        split_axis=0,
        concat_axis=0,
        tiled=True,
    )
    arrived = lax.all_gather(pieces, "tp", axis=2, tiled=True)
    expert_rows = arrived.reshape(-1, model_width)
    gate_pre = jnp.dot(expert_rows, expert_gate[0], preferred_element_type=jnp.float32)
    up_lin = jnp.dot(expert_rows, expert_up[0], preferred_element_type=jnp.float32)
    expert_act = (jax.nn.silu(gate_pre) * up_lin).astype(jnp.bfloat16)
    gathered_expert, gathered_shared = (
        lax.all_gather(expert_act, "tp", axis=1, tiled=True),
        lax.all_gather(shared_act, "tp", axis=1, tiled=True),
    )
    expert_out = jnp.dot(
        gathered_expert, expert_down[0], preferred_element_type=jnp.float32
    ).astype(jnp.bfloat16)
    returned = lax.all_to_all(
        expert_out.reshape(experts, capacity, col_width),
        "sp",
        split_axis=0,
        concat_axis=0,
        tiled=True,
    )
    returned = returned.reshape(experts * capacity, col_width)
    picked = returned[slot_dest].astype(jnp.float32).reshape(rows_here, top_count, col_width)
    routed = jnp.sum(picked * route_weight[:, :, None], axis=1)
    shared_cols = jnp.dot(gathered_shared, shared_down, preferred_element_type=jnp.float32)
    return (updated_cols.astype(jnp.float32) + shared_cols + routed).astype(jnp.bfloat16)


MESH = pl.DeviceIdType.MESH


def fused_kernel(
    dims,
    res_hbm,
    q_ref,
    k_ref,
    v_ref,
    seg_ref,
    routes_ref,
    rw_ref,
    sinks_ref,
    wo_hbm,
    gain_ref,
    eg_hbm,
    eu_hbm,
    ed_hbm,
    sg_hbm,
    su_hbm,
    sd_hbm,
    out_ref,
    res_v,
    wo_v,
    gu_v,
    sgu_v,
    dn_v,
    sdn_v,
    kh,
    vh,
    mh,
    marks_v,
    aux_rows,
    aux_ref,
    att,
    b1s,
    b1r,
    b2s,
    b2r,
    keep,
    upd,
    norm_v,
    act,
    eout,
    eback,
    acc,
    w_sem,
    halo_s,
    halo_r,
    b_s,
    b_r,
    u_s,
    u_r,
    a_s,
    a_r,
    e_s,
    e_r,
):
    rows, cols, width, window, hidden, heads, group = dims
    bf16, f32 = jnp.bfloat16, jnp.float32
    s = lax.axis_index("sp")
    t = lax.axis_index("tp")
    core = t % 2
    chip = t // 2
    mate = t + 1 - 2 * core
    over = t + 2 - 4 * chip
    diag = 3 - t

    def remote(src, dst, send, recv, sp, tp):
        return pltpu.make_async_remote_copy(
            src_ref=src,
            dst_ref=dst,
            send_sem=send,
            recv_sem=recv,
            device_id={"sp": sp, "tp": tp},
            device_id_type=MESH,
        )

    own_cols = pl.ds(pl.multiple_of(t * cols, cols), cols)
    loads = [
        pltpu.make_async_copy(wo_hbm, wo_v, w_sem.at[0]),
        pltpu.make_async_copy(res_hbm.at[:, own_cols], res_v, w_sem.at[1]),
        pltpu.make_async_copy(eg_hbm.at[0], gu_v.at[:, pl.ds(0, hidden)], w_sem.at[2]),
        pltpu.make_async_copy(eu_hbm.at[0], gu_v.at[:, pl.ds(hidden, hidden)], w_sem.at[3]),
        pltpu.make_async_copy(sg_hbm, sgu_v.at[:, pl.ds(0, hidden)], w_sem.at[4]),
        pltpu.make_async_copy(su_hbm, sgu_v.at[:, pl.ds(hidden, hidden)], w_sem.at[5]),
        pltpu.make_async_copy(ed_hbm.at[0], dn_v, w_sem.at[6]),
        pltpu.make_async_copy(sd_hbm, sdn_v, w_sem.at[7]),
    ]
    for load in loads:
        load.start()

    top_count = routes_ref.shape[0]
    aux_rows[...] = jnp.zeros_like(aux_rows)
    aux_rows[0:1, :] = seg_ref[...].astype(f32)
    aux_rows[1 : 1 + top_count, :] = routes_ref[...].astype(f32)
    aux_rows[1 + top_count : 1 + 2 * top_count, :] = rw_ref[...]
    marks_v[...] = jnp.broadcast_to(aux_rows[0:1, pl.ds(rows - window, window)], (8, window))
    barrier = pltpu.get_barrier_semaphore()
    pl.semaphore_signal(barrier, inc=1, device_id={"sp": s, "tp": mate}, device_id_type=MESH)
    pl.semaphore_signal(barrier, inc=1, device_id={"sp": s, "tp": over}, device_id_type=MESH)
    for step in range(1, 4):
        pl.semaphore_signal(
            barrier, inc=1, device_id={"sp": (s + step) % 4, "tp": t}, device_id_type=MESH
        )
    pl.semaphore_wait(barrier, 5)

    def marks_across(n):
        return aux_rows[0:1, pl.ds(n * window, window)]

    tail = pl.ds(rows - window, window)
    up_sp, down_sp = (s + 1) % 4, (s + 3) % 4
    halos = [
        remote(k_ref.at[tail], kh, halo_s.at[0], halo_r.at[0], up_sp, t),
        remote(v_ref.at[tail], vh, halo_s.at[1], halo_r.at[1], up_sp, t),
        remote(marks_v, mh, halo_s.at[2], halo_r.at[2], up_sp, t),
    ]

    @pl.when(s < 3)
    def _():
        for copy in halos:
            copy.start()

    @pl.when(s == 0)
    def _():
        kh[...] = jnp.zeros_like(kh)
        vh[...] = jnp.zeros_like(vh)
        mh[...] = jnp.full(mh.shape, -1.0, f32)

    for n in range(rows // window):
        here = pl.ds(n * window, window)
        aux_ref[here, :] = jnp.transpose(aux_rows[:, here])

    q_pos = lax.broadcasted_iota(jnp.int32, (window, window), 0)
    k_pos = lax.broadcasted_iota(jnp.int32, (window, window), 1)

    def attend(n):
        here = pl.ds(n * window, window)
        if n == 0:
            k_prev, v_prev, m_prev = kh[...], vh[...], mh[0:1, :]
        else:
            before = pl.ds((n - 1) * window, window)
            k_prev, v_prev, m_prev = k_ref[before, :], v_ref[before, :], marks_across(n - 1)
        k_own, v_own, m_own = k_ref[here, :], v_ref[here, :], marks_across(n)
        marks = aux_ref[here, 0:1]
        ok_prev = (k_pos > q_pos) & (marks == m_prev)
        ok_own = (k_pos <= q_pos) & (marks == m_own)
        for h in range(heads):
            kv = slice((h // group) * HEAD_DIM, (h // group + 1) * HEAD_DIM)
            qh = q_ref[here, h * HEAD_DIM : (h + 1) * HEAD_DIM]
            contract = (((1,), (1,)), ((), ()))
            sc_prev = lax.dot_general(
                qh, k_prev[:, kv], contract, preferred_element_type=f32
            ) * HEAD_DIM ** (-0.5)
            sc_own = lax.dot_general(
                qh, k_own[:, kv], contract, preferred_element_type=f32
            ) * HEAD_DIM ** (-0.5)
            sc_prev = jnp.where(ok_prev, sc_prev, -jnp.inf)
            sc_own = jnp.where(ok_own, sc_own, -jnp.inf)
            sink = sinks_ref[h]
            top = jnp.maximum(
                jnp.max(jnp.maximum(sc_prev, sc_own), axis=-1, keepdims=True), sink
            )
            ex_prev = jnp.exp(sc_prev - top)
            ex_own = jnp.exp(sc_own - top)
            total = jnp.sum(ex_prev + ex_own, axis=-1, keepdims=True) + jnp.exp(sink - top)
            p_prev = (ex_prev / total).astype(bf16)
            p_own = (ex_own / total).astype(bf16)
            got = jnp.dot(p_prev, v_prev[:, kv], preferred_element_type=f32) + jnp.dot(
                p_own, v_own[:, kv], preferred_element_type=f32
            )
            att[here, h * HEAD_DIM : (h + 1) * HEAD_DIM] = got.astype(bf16)

    def project(n, chunk):
        where = pl.ds(pl.multiple_of(chunk * cols, cols), cols)
        return jnp.dot(
            att[pl.ds(n * window, window), :], wo_v[:, where], preferred_element_type=f32
        )

    halves = list(range(rows // window))[::-1]
    pending = []
    first = {}
    for n in halves:
        if n == 0:

            @pl.when(s > 0)
            def _():
                for copy in halos:
                    copy.wait_recv()

        attend(n)
        if n == halves[0]:
            loads[0].wait()
        for far in (1, 0):
            chunk = (over if far else t) + 1 - 2 * core
            b1s[n, far] = project(n, chunk).astype(bf16)
            copy = remote(
                b1s.at[n, far], b1r.at[n, far], b_s.at[n, far], b_r.at[n, far], s, mate
            )
            copy.start()
            pending.append(copy)
            first[n, far] = copy
    second = {}
    for n in halves:
        mine = project(n, over)
        first[n, 1].wait_recv()
        b2s[n] = (mine + b1r[n, 1].astype(f32)).astype(bf16)
        copy = remote(b2s.at[n], b2r.at[n], b_s.at[n, 2], b_r.at[n, 2], s, over)
        copy.start()
        pending.append(copy)
        second[n] = copy
    loads[1].wait()
    for n in halves:
        here = pl.ds(n * window, window)
        mine = project(n, t) + res_v[here, :].astype(f32)
        first[n, 0].wait_recv()
        keep[here, :] = mine + b1r[n, 0].astype(f32)

    def piece(b, chunk, n):
        return upd.at[b, chunk, pl.ds(n * window, window)]

    def share(kind, k, b, chunk, n, sp, tp):
        return remote(
            piece(b, chunk, n),
            piece(b, chunk, n),
            u_s.at[kind, k, n],
            u_r.at[b, chunk, n],
            sp,
            tp,
        )

    conditional = []
    for n in halves:
        here = pl.ds(n * window, window)
        second[n].wait_recv()
        upd[s, t, here, :] = (keep[here, :] + b2r[n].astype(f32)).astype(bf16)
        over_copy = share(3, 0, s, t, n, s, over)
        over_copy.start()
        up_copy = share(0, 0, s, t, n, up_sp, t)
        down_copy = share(1, 0, s, t, n, down_sp, t)

        @pl.when(s < 3)
        def _():
            up_copy.start()

        @pl.when(s > 0)
        def _():
            down_copy.start()

        mate_copy = share(2, 0, s, t, n, s, mate)
        mate_copy.start()
        pending += [over_copy, mate_copy]
        conditional += [(s < 3, up_copy), (s > 0, down_copy)]

    side = s // 2
    edge = s + side * (3 - 2 * s)
    order = [s]
    for k in range(1, 4):
        flat = (k, k + edge, k - 2 * edge, k)[k]
        order.append(flat + side * (3 - 2 * flat))

    def arrive(k):
        b = order[k]
        for n in halves:
            share(0, k, b, t, n, s, mate).wait_recv()
            copy = share(3, k, b, t, n, s, over)
            copy.start()
            to_up = share(0, k, b, t, n, up_sp, t)
            to_down = share(1, k, b, t, n, down_sp, t)
            rising = (b < s) & (s < 3)
            falling = (b > s) & (s > 0)

            @pl.when(rising)
            def _():
                to_up.start()

            @pl.when(falling)
            def _():
                to_down.start()

            conditional.extend([(rising, to_up), (falling, to_down)])
            mate_copy = share(2, k, b, t, n, s, mate)
            mate_copy.start()
            pending.extend([copy, mate_copy])

    def relay(k):
        b = order[k]
        for n in halves:
            share(4, k, b, over, n, s, mate).wait_recv()
            copy = share(4, k, b, over, n, s, mate)
            copy.start()
            pending.append(copy)

    def normalize(k):
        b = order[k]
        for n in halves:
            share(2, k, b, mate, n, s, mate).wait_recv()
            share(4, k, b, diag, n, s, mate).wait_recv()
        step = 32

        def body(i, carry):
            here = pl.ds(pl.multiple_of(i * step, step), step)
            squares = jnp.zeros((step, 1), f32)
            for chunk in range(4):
                part = upd[b, chunk, here, :].astype(f32)
                squares = squares + jnp.sum(part * part, axis=-1, keepdims=True)
            inv = lax.rsqrt(squares / width + epsilon)
            for chunk in range(4):
                part = upd[b, chunk, here, :].astype(f32)
                span = slice(chunk * cols, (chunk + 1) * cols)
                norm_v[here, span] = (part * inv * gain_ref[0:1, span]).astype(bf16)
            return carry

        lax.fori_loop(0, rows // step, body, 0)

    def pass_on(slot, kind, chunk, tp):
        return remote(
            act.at[slot, chunk],
            act.at[slot, chunk],
            a_s.at[kind, slot],
            a_r.at[slot, chunk],
            s,
            tp,
        )

    def activate(slot, weight):
        both = jnp.dot(norm_v[...], weight[...], preferred_element_type=f32)
        gate, lin = both[:, :hidden], both[:, hidden:]
        act[slot, t] = (gate / (1.0 + jnp.exp(-gate)) * lin).astype(bf16)
        for kind, tp in ((0, over), (1, mate)):
            copy = pass_on(slot, kind, t, tp)
            copy.start()
            pending.append(copy)

    def relay_act(slot):
        pass_on(slot, 2, over, mate).wait_recv()
        copy = pass_on(slot, 2, over, mate)
        copy.start()
        pending.append(copy)

    def contract_act(slot, weight):
        pass_on(slot, 1, mate, mate).wait_recv()
        pass_on(slot, 2, diag, mate).wait_recv()
        total = None
        for chunk in range(4):
            part = jnp.dot(
                act[slot, chunk],
                weight[chunk * hidden : (chunk + 1) * hidden, :],
                preferred_element_type=f32,
            )
            total = part if total is None else total + part
        return total


    def finish(k):
        eout[k] = contract_act(k, dn_v).astype(bf16)
        copy = remote(eout.at[k], eback.at[s], e_s.at[k], e_r.at[s], order[k], t)
        copy.start()
        pending.append(copy)

    arrive(1)
    relay(0)
    arrive(2)
    relay(1)
    loads[2].wait()
    loads[3].wait()
    normalize(1)
    activate(1, gu_v)
    arrive(3)
    relay(2)
    normalize(2)
    activate(2, gu_v)
    relay_act(1)
    loads[6].wait()
    finish(1)
    relay(3)
    normalize(3)
    activate(3, gu_v)
    relay_act(2)
    finish(2)
    normalize(0)
    activate(0, gu_v)
    loads[4].wait()
    loads[5].wait()
    activate(4, sgu_v)
    relay_act(3)
    finish(3)
    relay_act(0)
    relay_act(4)
    eout[0] = contract_act(0, dn_v).astype(bf16)
    loads[7].wait()
    acc[...] = contract_act(4, sdn_v)

    def weight_of(e):
        total = jnp.zeros((rows, 1), f32)
        for k in range(1, top_count + 1):
            weight = aux_ref[:, top_count + k : top_count + k + 1]
            named = aux_ref[:, k : k + 1] == jnp.full((rows, 1), e, jnp.int32).astype(f32)
            total = total + jnp.where(named, weight, 0.0)
        return total

    acc[...] = (
        acc[...]
        + upd[s, t].astype(f32)
        + weight_of(s) * eout[0].astype(f32)
    )
    for k in range(1, 4):
        b = order[k]
        remote(eout.at[k], eback.at[b], e_s.at[k], e_r.at[b], b, t).wait_recv()
        acc[...] = acc[...] + weight_of(b) * eback[b].astype(f32)
    out_ref[...] = acc[...].astype(bf16)

    for copy in pending:
        copy.wait_send()
    for when, copy in conditional:

        @pl.when(when)
        def _():
            copy.wait_send()

    @pl.when(s < 3)
    def _():
        for copy in halos:
            copy.wait_send()


def layer(
    residual,
    queries,
    keys,
    values,
    segments,
    routes,
    route_weight,
    sinks,
    out_weight,
    norm_gain,
    expert_gate,
    expert_up,
    expert_down,
    shared_gate,
    shared_up,
    shared_down,
):
    arguments = (
        residual,
        queries,
        keys,
        values,
        segments,
        routes,
        route_weight,
        sinks,
        out_weight,
        norm_gain,
        expert_gate,
        expert_up,
        expert_down,
        shared_gate,
        shared_up,
        shared_down,
    )
    rows, width = residual.shape
    n_sp, n_tp = lax.axis_size("sp"), lax.axis_size("tp")
    capacity = 2 * rows * routes.shape[1] // n_sp
    hidden = expert_gate.shape[2]
    if n_sp != 4 or n_tp != 4 or capacity < rows or shared_gate.shape[1] != hidden:
        return shards(*arguments)
    cols = width // n_tp
    heads = queries.shape[1] // HEAD_DIM
    group = queries.shape[1] // keys.shape[1]
    kv_width = keys.shape[1]
    blocks = rows // WINDOW
    bf16, f32 = jnp.bfloat16, jnp.float32
    vmem = pl.BlockSpec(memory_space=pltpu.VMEM)
    anywhere = pl.BlockSpec(memory_space=pl.ANY)
    dma = pltpu.SemaphoreType.DMA
    return pl.pallas_call(
        functools.partial(fused_kernel, (rows, cols, width, WINDOW, hidden, heads, group)),
        out_shape=jax.ShapeDtypeStruct((rows, cols), bf16),
        in_specs=[anywhere]
        + [vmem] * 6
        + [pl.BlockSpec(memory_space=pltpu.SMEM), anywhere, vmem]
        + [anywhere] * 6,
        out_specs=vmem,
        scratch_shapes=[
            pltpu.VMEM((rows, cols), bf16),
            pltpu.VMEM(out_weight.shape, bf16),
            pltpu.VMEM((width, 2 * hidden), bf16),
            pltpu.VMEM((width, 2 * hidden), bf16),
            pltpu.VMEM(expert_down.shape[1:], bf16),
            pltpu.VMEM(shared_down.shape, bf16),
            pltpu.VMEM((WINDOW, kv_width), bf16),
            pltpu.VMEM((WINDOW, kv_width), bf16),
            pltpu.VMEM((8, WINDOW), f32),
            pltpu.VMEM((8, WINDOW), f32),
            pltpu.VMEM((WINDOW, rows), f32),
            pltpu.VMEM((rows, WINDOW), f32),
            pltpu.VMEM((rows, heads * HEAD_DIM), bf16),
            pltpu.VMEM((blocks, 2, WINDOW, cols), bf16),
            pltpu.VMEM((blocks, 2, WINDOW, cols), bf16),
            pltpu.VMEM((blocks, WINDOW, cols), bf16),
            pltpu.VMEM((blocks, WINDOW, cols), bf16),
            pltpu.VMEM((rows, cols), f32),
            pltpu.VMEM((4, 4, rows, cols), bf16),
            pltpu.VMEM((rows, width), bf16),
            pltpu.VMEM((5, 4, rows, hidden), bf16),
            pltpu.VMEM((4, rows, cols), bf16),
            pltpu.VMEM((4, rows, cols), bf16),
            pltpu.VMEM((rows, cols), f32),
            dma((8,)),
            dma((3,)),
            dma((3,)),
            dma((blocks, 3)),
            dma((blocks, 3)),
            dma((5, 4, blocks)),
            dma((4, 4, blocks)),
            dma((3, 5)),
            dma((5, 4)),
            dma((4,)),
            dma((4,)),
        ],
        compiler_params=pltpu.CompilerParams(collective_id=0, has_side_effects=True),
    )(
        residual,
        queries,
        keys,
        values,
        segments[None, :],
        routes.T,
        route_weight.T,
        sinks,
        out_weight,
        norm_gain[None, :],
        expert_gate,
        expert_up,
        expert_down,
        shared_gate,
        shared_up,
        shared_down,
    )


def solution(mesh):
    placed = (
        P(("grp", "sp"), None),
        P(("grp", "sp"), "tp"),
        P(("grp", "sp"), "tp"),
        P(("grp", "sp"), "tp"),
        P(("grp", "sp")),
        P(("grp", "sp"), None),
        P(("grp", "sp"), None),
        P("tp"),
        P("tp", None),
        P(),
        P("sp", None, "tp"),
        P("sp", None, "tp"),
        P("sp", None, "tp"),
        P(None, "tp"),
        P(None, "tp"),
        P(None, "tp"),
    )
    return jax.shard_map(
        layer, mesh=mesh, in_specs=placed, out_specs=P(("grp", "sp"), "tp"), check_vma=False
    )
```

```python
import functools
import jax
import jax.numpy as jnp
from jax import lax
from jax.experimental import pallas as pl
from jax.experimental.pallas import tpu as pltpu
from jax.sharding import PartitionSpec as P

HEAD_DIM = 64
WINDOW = 128


epsilon = 1e-06


def passed_along(value, axis, steps):
    count = lax.axis_size(axis)
    leading, last = (max(0, -steps), min(count, count - steps))
    return lax.ppermute(value, axis, [(source, source + steps) for source in range(leading, last)])


def banded(prev_rows, own_rows, window_len):
    blocks = own_rows.shape[0] // window_len
    joined = jnp.concatenate([prev_rows, own_rows], axis=0)
    shaped = joined.reshape((blocks + 1, window_len) + own_rows.shape[1:])
    return jnp.concatenate([shaped[:-1], shaped[1:]], axis=1)


def shards(
    residual,
    queries,
    keys,
    values,
    segments,
    routes,
    route_weight,
    sinks,
    out_weight,
    norm_gain,
    expert_gate,
    expert_up,
    expert_down,
    shared_gate,
    shared_up,
    shared_down,
):
    rows_here = residual.shape[0]
    model_width = residual.shape[1]
    tp_count = lax.axis_size("tp")
    tp_index = lax.axis_index("tp")
    head_local = queries.shape[1] // HEAD_DIM
    kv_local = keys.shape[1] // HEAD_DIM
    group_size = head_local // kv_local
    window_len = WINDOW
    blocks = rows_here // window_len
    own_marks = (segments % 256 + 1).astype(jnp.bfloat16)
    prev_keys, prev_values, prev_marks = passed_along(
        (
            keys[rows_here - window_len :],
            values[rows_here - window_len :],
            own_marks[rows_here - window_len :],
        ),
        "sp",
        1,
    )
    key_band = banded(prev_keys, keys, window_len).reshape(
        blocks, 2 * window_len, kv_local, HEAD_DIM
    )
    value_band = banded(prev_values, values, window_len).reshape(
        blocks, 2 * window_len, kv_local, HEAD_DIM
    )
    mark_band = banded(prev_marks, own_marks, window_len).astype(jnp.float32)
    query_marks = own_marks.reshape(blocks, window_len).astype(jnp.float32)
    query_blocks = queries.reshape(blocks, window_len, kv_local, group_size, HEAD_DIM)
    scores = jnp.einsum(
        "nqhgd,nkhd->nhgqk", query_blocks, key_band, preferred_element_type=jnp.float32
    ) * HEAD_DIM ** (-0.5)
    offsets = jnp.arange(window_len)[:, None] + window_len - jnp.arange(2 * window_len)[None, :]
    allowed = (
        (offsets >= 0) & (offsets < window_len) & (query_marks[:, :, None] == mark_band[:, None, :])
    )
    sink_logits = sinks.reshape(kv_local, group_size)[None, :, :, None]
    masked = jnp.where(allowed[:, None, None], scores, -jnp.inf)
    top_score = jnp.maximum(jnp.max(masked, axis=-1), sink_logits)
    exp_terms = jnp.where(allowed[:, None, None], jnp.exp(scores - top_score[..., None]), 0.0)
    denominator = jnp.sum(exp_terms, axis=-1) + jnp.exp(sink_logits - top_score)
    probabilities = (exp_terms / denominator[..., None]).astype(jnp.bfloat16)
    attended = jnp.einsum(
        "nhgqk,nkhd->nqhgd", probabilities, value_band, preferred_element_type=jnp.float32
    )
    attended = attended.astype(jnp.bfloat16).reshape(rows_here, head_local * HEAD_DIM)
    partial_value = jnp.dot(attended, out_weight, preferred_element_type=jnp.float32)
    col_width = model_width // tp_count
    col_start = tp_index * col_width
    summed = lax.psum(partial_value, "tp")
    updated = (residual.astype(jnp.float32) + summed).astype(jnp.bfloat16)
    updated_f32 = updated.astype(jnp.float32)
    inv_rms = lax.rsqrt(jnp.mean(updated_f32 * updated_f32, axis=-1, keepdims=True) + epsilon)
    normed = (updated_f32 * inv_rms * norm_gain).astype(jnp.bfloat16)
    updated_cols = lax.dynamic_slice_in_dim(updated, col_start, col_width, 1)
    normed_cols = lax.dynamic_slice_in_dim(normed, col_start, col_width, 1)
    shared_pre = jnp.dot(normed, shared_gate, preferred_element_type=jnp.float32)
    shared_lin = jnp.dot(normed, shared_up, preferred_element_type=jnp.float32)
    shared_act = (jax.nn.silu(shared_pre) * shared_lin).astype(jnp.bfloat16)
    top_count = routes.shape[1]
    experts = lax.axis_size("sp")
    capacity = 2 * rows_here * top_count // experts
    flat_ids = routes.reshape(-1)
    one_hot = (flat_ids[:, None] == jnp.arange(experts, dtype=jnp.int32)[None, :]).astype(jnp.int32)
    rank_in = jnp.cumsum(one_hot, axis=0) - one_hot
    slot_dest = flat_ids * capacity + jnp.sum(rank_in * one_hot, axis=1)
    token_of = jnp.arange(rows_here * top_count, dtype=jnp.int32) // top_count
    slot_token = jnp.full((experts * capacity,), -1, jnp.int32).at[slot_dest].set(token_of)
    filled = slot_token >= 0
    safe_token = jnp.where(filled, slot_token, 0)
    outgoing = jnp.where(filled[:, None], normed_cols[safe_token], jnp.zeros((), jnp.bfloat16))
    pieces = lax.all_to_all(
        outgoing.reshape(experts, capacity, col_width),
        "sp",
        split_axis=0,
        concat_axis=0,
        tiled=True,
    )
    arrived = lax.all_gather(pieces, "tp", axis=2, tiled=True)
    expert_rows = arrived.reshape(-1, model_width)
    gate_pre = jnp.dot(expert_rows, expert_gate[0], preferred_element_type=jnp.float32)
    up_lin = jnp.dot(expert_rows, expert_up[0], preferred_element_type=jnp.float32)
    expert_act = (jax.nn.silu(gate_pre) * up_lin).astype(jnp.bfloat16)
    gathered_expert, gathered_shared = (
        lax.all_gather(expert_act, "tp", axis=1, tiled=True),
        lax.all_gather(shared_act, "tp", axis=1, tiled=True),
    )
    expert_out = jnp.dot(
        gathered_expert, expert_down[0], preferred_element_type=jnp.float32
    ).astype(jnp.bfloat16)
    returned = lax.all_to_all(
        expert_out.reshape(experts, capacity, col_width),
        "sp",
        split_axis=0,
        concat_axis=0,
        tiled=True,
    )
    returned = returned.reshape(experts * capacity, col_width)
    picked = returned[slot_dest].astype(jnp.float32).reshape(rows_here, top_count, col_width)
    routed = jnp.sum(picked * route_weight[:, :, None], axis=1)
    shared_cols = jnp.dot(gathered_shared, shared_down, preferred_element_type=jnp.float32)
    return (updated_cols.astype(jnp.float32) + shared_cols + routed).astype(jnp.bfloat16)


MESH = pl.DeviceIdType.MESH


def fused_kernel(
    dims,
    res_hbm,
    q_ref,
    k_ref,
    v_ref,
    seg_ref,
    routes_ref,
    rw_ref,
    sinks_ref,
    wo_hbm,
    gain_ref,
    eg_hbm,
    eu_hbm,
    ed_hbm,
    sg_hbm,
    su_hbm,
    sd_hbm,
    out_ref,
    res_v,
    wo_v,
    gu_v,
    sgu_v,
    dn_v,
    sdn_v,
    kh,
    vh,
    mh,
    marks_v,
    aux_rows,
    aux_ref,
    att,
    b1s,
    b1r,
    b2s,
    b2r,
    keep,
    upd,
    norm_v,
    act,
    eout,
    eback,
    acc,
    w_sem,
    halo_s,
    halo_r,
    b_s,
    b_r,
    u_s,
    u_r,
    a_s,
    a_r,
    e_s,
    e_r,
):
    rows, cols, width, window, hidden, heads, group = dims
    bf16, f32 = jnp.bfloat16, jnp.float32
    s = lax.axis_index("sp")
    t = lax.axis_index("tp")
    core = t % 2
    chip = t // 2
    mate = t + 1 - 2 * core
    over = t + 2 - 4 * chip
    diag = 3 - t

    def remote(src, dst, send, recv, sp, tp):
        return pltpu.make_async_remote_copy(
            src_ref=src,
            dst_ref=dst,
            send_sem=send,
            recv_sem=recv,
            device_id={"sp": sp, "tp": tp},
            device_id_type=MESH,
        )

    own_cols = pl.ds(pl.multiple_of(t * cols, cols), cols)
    loads = [
        pltpu.make_async_copy(wo_hbm, wo_v, w_sem.at[0]),
        pltpu.make_async_copy(res_hbm.at[:, own_cols], res_v, w_sem.at[1]),
        pltpu.make_async_copy(eg_hbm.at[0], gu_v.at[:, pl.ds(0, hidden)], w_sem.at[2]),
        pltpu.make_async_copy(eu_hbm.at[0], gu_v.at[:, pl.ds(hidden, hidden)], w_sem.at[3]),
        pltpu.make_async_copy(sg_hbm, sgu_v.at[:, pl.ds(0, hidden)], w_sem.at[4]),
        pltpu.make_async_copy(su_hbm, sgu_v.at[:, pl.ds(hidden, hidden)], w_sem.at[5]),
        pltpu.make_async_copy(ed_hbm.at[0], dn_v, w_sem.at[6]),
        pltpu.make_async_copy(sd_hbm, sdn_v, w_sem.at[7]),
    ]
    for load in loads:
        load.start()

    top_count = routes_ref.shape[0]
    aux_rows[...] = jnp.zeros_like(aux_rows)
    aux_rows[0:1, :] = seg_ref[...].astype(f32)
    aux_rows[1 : 1 + top_count, :] = routes_ref[...].astype(f32)
    aux_rows[1 + top_count : 1 + 2 * top_count, :] = rw_ref[...]
    marks_v[...] = jnp.broadcast_to(aux_rows[0:1, pl.ds(rows - window, window)], (8, window))
    barrier = pltpu.get_barrier_semaphore()
    pl.semaphore_signal(barrier, inc=1, device_id={"sp": s, "tp": mate}, device_id_type=MESH)
    pl.semaphore_signal(barrier, inc=1, device_id={"sp": s, "tp": over}, device_id_type=MESH)
    for step in range(1, 4):
        pl.semaphore_signal(
            barrier, inc=1, device_id={"sp": (s + step) % 4, "tp": t}, device_id_type=MESH
        )
    pl.semaphore_wait(barrier, 5)

    def marks_across(n):
        return aux_rows[0:1, pl.ds(n * window, window)]

    tail = pl.ds(rows - window, window)
    up_sp, down_sp = (s + 1) % 4, (s + 3) % 4
    halos = [
        remote(k_ref.at[tail], kh, halo_s.at[0], halo_r.at[0], up_sp, t),
        remote(v_ref.at[tail], vh, halo_s.at[1], halo_r.at[1], up_sp, t),
        remote(marks_v, mh, halo_s.at[2], halo_r.at[2], up_sp, t),
    ]

    @pl.when(s < 3)
    def _():
        for copy in halos:
            copy.start()

    @pl.when(s == 0)
    def _():
        kh[...] = jnp.zeros_like(kh)
        vh[...] = jnp.zeros_like(vh)
        mh[...] = jnp.full(mh.shape, -1.0, f32)

    for n in range(rows // window):
        here = pl.ds(n * window, window)
        aux_ref[here, :] = jnp.transpose(aux_rows[:, here])

    q_pos = lax.broadcasted_iota(jnp.int32, (window, window), 0)
    k_pos = lax.broadcasted_iota(jnp.int32, (window, window), 1)

    def attend(n):
        here = pl.ds(n * window, window)
        if n == 0:
            k_prev, v_prev, m_prev = kh[...], vh[...], mh[0:1, :]
        else:
            before = pl.ds((n - 1) * window, window)
            k_prev, v_prev, m_prev = k_ref[before, :], v_ref[before, :], marks_across(n - 1)
        k_own, v_own, m_own = k_ref[here, :], v_ref[here, :], marks_across(n)
        marks = aux_ref[here, 0:1]
        ok_prev = (k_pos > q_pos) & (marks == m_prev)
        ok_own = (k_pos <= q_pos) & (marks == m_own)
        for h in range(heads):
            kv = slice((h // group) * HEAD_DIM, (h // group + 1) * HEAD_DIM)
            qh = q_ref[here, h * HEAD_DIM : (h + 1) * HEAD_DIM]
            contract = (((1,), (1,)), ((), ()))
            sc_prev = lax.dot_general(
                qh, k_prev[:, kv], contract, preferred_element_type=f32
            ) * HEAD_DIM ** (-0.5)
            sc_own = lax.dot_general(
                qh, k_own[:, kv], contract, preferred_element_type=f32
            ) * HEAD_DIM ** (-0.5)
            sc_prev = jnp.where(ok_prev, sc_prev, -jnp.inf)
            sc_own = jnp.where(ok_own, sc_own, -jnp.inf)
            sink = sinks_ref[h]
            top = jnp.maximum(
                jnp.max(jnp.maximum(sc_prev, sc_own), axis=-1, keepdims=True), sink
            )
            ex_prev = jnp.exp(sc_prev - top)
            ex_own = jnp.exp(sc_own - top)
            total = jnp.sum(ex_prev + ex_own, axis=-1, keepdims=True) + jnp.exp(sink - top)
            p_prev = (ex_prev / total).astype(bf16)
            p_own = (ex_own / total).astype(bf16)
            got = jnp.dot(p_prev, v_prev[:, kv], preferred_element_type=f32) + jnp.dot(
                p_own, v_own[:, kv], preferred_element_type=f32
            )
            att[here, h * HEAD_DIM : (h + 1) * HEAD_DIM] = got.astype(bf16)

    def project(n, chunk):
        where = pl.ds(pl.multiple_of(chunk * cols, cols), cols)
        return jnp.dot(
            att[pl.ds(n * window, window), :], wo_v[:, where], preferred_element_type=f32
        )

    halves = list(range(rows // window))[::-1]
    pending = []
    first = {}
    for n in halves:
        if n == 0:

            @pl.when(s > 0)
            def _():
                for copy in halos:
                    copy.wait_recv()

        attend(n)
        if n == halves[0]:
            loads[0].wait()
        for far in (1, 0):
            chunk = (over if far else t) + 1 - 2 * core
            b1s[n, far] = project(n, chunk).astype(bf16)
            copy = remote(
                b1s.at[n, far], b1r.at[n, far], b_s.at[n, far], b_r.at[n, far], s, mate
            )
            copy.start()
            pending.append(copy)
            first[n, far] = copy
    second = {}
    for n in halves:
        mine = project(n, over)
        first[n, 1].wait_recv()
        b2s[n] = (mine + b1r[n, 1].astype(f32)).astype(bf16)
        copy = remote(b2s.at[n], b2r.at[n], b_s.at[n, 2], b_r.at[n, 2], s, over)
        copy.start()
        pending.append(copy)
        second[n] = copy
    loads[1].wait()
    for n in halves:
        here = pl.ds(n * window, window)
        mine = project(n, t) + res_v[here, :].astype(f32)
        first[n, 0].wait_recv()
        keep[here, :] = mine + b1r[n, 0].astype(f32)

    def piece(b, chunk, n):
        return upd.at[b, chunk, pl.ds(n * window, window)]

    def share(kind, k, b, chunk, n, sp, tp):
        return remote(
            piece(b, chunk, n),
            piece(b, chunk, n),
            u_s.at[kind, k, n],
            u_r.at[b, chunk, n],
            sp,
            tp,
        )

    conditional = []
    for n in halves:
        here = pl.ds(n * window, window)
        second[n].wait_recv()
        upd[s, t, here, :] = (keep[here, :] + b2r[n].astype(f32)).astype(bf16)
        over_copy = share(3, 0, s, t, n, s, over)
        over_copy.start()
        up_copy = share(0, 0, s, t, n, up_sp, t)
        down_copy = share(1, 0, s, t, n, down_sp, t)

        @pl.when(s < 3)
        def _():
            up_copy.start()

        @pl.when(s > 0)
        def _():
            down_copy.start()

        mate_copy = share(2, 0, s, t, n, s, mate)
        mate_copy.start()
        pending += [over_copy, mate_copy]
        conditional += [(s < 3, up_copy), (s > 0, down_copy)]

    side = s // 2
    edge = s + side * (3 - 2 * s)
    order = [s]
    for k in range(1, 4):
        flat = (k, k + edge, k - 2 * edge, k)[k]
        order.append(flat + side * (3 - 2 * flat))

    along = halves[:1]

    def onward(k, kinds, chunk, n):
        b = order[k]
        to_up = share(kinds[0], k, b, chunk, n, up_sp, t)
        to_down = share(kinds[1], k, b, chunk, n, down_sp, t)
        rising = s < 3 if k == 0 else (b < s) & (s < 3)
        falling = s > 0 if k == 0 else (b > s) & (s > 0)

        @pl.when(rising)
        def _():
            to_up.start()

        @pl.when(falling)
        def _():
            to_down.start()

        conditional.extend([(rising, to_up), (falling, to_down)])

    def arrive(k):
        b = order[k]
        for n in halves:
            share(0, k, b, t, n, s, mate).wait_recv()
            onward(k, (0, 1), t, n)
            if n not in along:
                copy = share(3, k, b, t, n, s, over)
                copy.start()
                pending.append(copy)
            mate_copy = share(2, k, b, t, n, s, mate)
            mate_copy.start()
            pending.append(mate_copy)

    def relay_half(k, n):
        b = order[k]
        share(4, k, b, over, n, s, mate).wait_recv()
        if n in along:
            onward(k, (5, 6), over, n)
        copy = share(4, k, b, over, n, s, mate)
        copy.start()
        pending.append(copy)

    def relay(k):
        for n in halves:
            if k == 0 or n not in along:
                relay_half(k, n)

    def arrive_over(k):
        for n in along:
            relay_half(k, n)

    def normalize(k):
        b = order[k]
        for n in halves:
            share(2, k, b, mate, n, s, mate).wait_recv()
            share(4, k, b, diag, n, s, mate).wait_recv()
        step = 32

        def body(i, carry):
            here = pl.ds(pl.multiple_of(i * step, step), step)
            squares = jnp.zeros((step, 1), f32)
            for chunk in range(4):
                part = upd[b, chunk, here, :].astype(f32)
                squares = squares + jnp.sum(part * part, axis=-1, keepdims=True)
            inv = lax.rsqrt(squares / width + epsilon)
            for chunk in range(4):
                part = upd[b, chunk, here, :].astype(f32)
                span = slice(chunk * cols, (chunk + 1) * cols)
                norm_v[here, span] = (part * inv * gain_ref[0:1, span]).astype(bf16)
            return carry

        lax.fori_loop(0, rows // step, body, 0)

    def pass_on(slot, kind, chunk, tp):
        return remote(
            act.at[slot, chunk],
            act.at[slot, chunk],
            a_s.at[kind, slot],
            a_r.at[slot, chunk],
            s,
            tp,
        )

    def activate(slot, weight):
        both = jnp.dot(norm_v[...], weight[...], preferred_element_type=f32)
        gate, lin = both[:, :hidden], both[:, hidden:]
        act[slot, t] = (gate / (1.0 + jnp.exp(-gate)) * lin).astype(bf16)
        for kind, tp in ((0, over), (1, mate)):
            copy = pass_on(slot, kind, t, tp)
            copy.start()
            pending.append(copy)

    def relay_act(slot):
        pass_on(slot, 2, over, mate).wait_recv()
        copy = pass_on(slot, 2, over, mate)
        copy.start()
        pending.append(copy)

    def contract_act(slot, weight):
        pass_on(slot, 1, mate, mate).wait_recv()
        pass_on(slot, 2, diag, mate).wait_recv()
        total = None
        for chunk in range(4):
            part = jnp.dot(
                act[slot, chunk],
                weight[chunk * hidden : (chunk + 1) * hidden, :],
                preferred_element_type=f32,
            )
            total = part if total is None else total + part
        return total


    def finish(k):
        eout[k] = contract_act(k, dn_v).astype(bf16)
        copy = remote(eout.at[k], eback.at[s], e_s.at[k], e_r.at[s], order[k], t)
        copy.start()
        pending.append(copy)

    arrive(1)
    relay(0)
    arrive(2)
    arrive_over(1)
    relay(1)
    loads[2].wait()
    loads[3].wait()
    normalize(1)
    activate(1, gu_v)
    arrive(3)
    arrive_over(2)
    relay(2)
    normalize(2)
    activate(2, gu_v)
    relay_act(1)
    loads[6].wait()
    finish(1)
    arrive_over(3)
    relay(3)
    normalize(3)
    activate(3, gu_v)
    relay_act(2)
    finish(2)
    normalize(0)
    activate(0, gu_v)
    loads[4].wait()
    loads[5].wait()
    activate(4, sgu_v)
    relay_act(3)
    finish(3)
    relay_act(0)
    relay_act(4)
    eout[0] = contract_act(0, dn_v).astype(bf16)
    loads[7].wait()
    acc[...] = contract_act(4, sdn_v)

    def weight_of(e):
        total = jnp.zeros((rows, 1), f32)
        for k in range(1, top_count + 1):
            weight = aux_ref[:, top_count + k : top_count + k + 1]
            named = aux_ref[:, k : k + 1] == jnp.full((rows, 1), e, jnp.int32).astype(f32)
            total = total + jnp.where(named, weight, 0.0)
        return total

    acc[...] = (
        acc[...]
        + upd[s, t].astype(f32)
        + weight_of(s) * eout[0].astype(f32)
    )
    for k in range(1, 4):
        b = order[k]
        remote(eout.at[k], eback.at[b], e_s.at[k], e_r.at[b], b, t).wait_recv()
        acc[...] = acc[...] + weight_of(b) * eback[b].astype(f32)
    out_ref[...] = acc[...].astype(bf16)

    for copy in pending:
        copy.wait_send()
    for when, copy in conditional:

        @pl.when(when)
        def _():
            copy.wait_send()

    @pl.when(s < 3)
    def _():
        for copy in halos:
            copy.wait_send()


def layer(
    residual,
    queries,
    keys,
    values,
    segments,
    routes,
    route_weight,
    sinks,
    out_weight,
    norm_gain,
    expert_gate,
    expert_up,
    expert_down,
    shared_gate,
    shared_up,
    shared_down,
):
    arguments = (
        residual,
        queries,
        keys,
        values,
        segments,
        routes,
        route_weight,
        sinks,
        out_weight,
        norm_gain,
        expert_gate,
        expert_up,
        expert_down,
        shared_gate,
        shared_up,
        shared_down,
    )
    rows, width = residual.shape
    n_sp, n_tp = lax.axis_size("sp"), lax.axis_size("tp")
    capacity = 2 * rows * routes.shape[1] // n_sp
    hidden = expert_gate.shape[2]
    if n_sp != 4 or n_tp != 4 or capacity < rows or shared_gate.shape[1] != hidden:
        return shards(*arguments)
    cols = width // n_tp
    heads = queries.shape[1] // HEAD_DIM
    group = queries.shape[1] // keys.shape[1]
    kv_width = keys.shape[1]
    blocks = rows // WINDOW
    bf16, f32 = jnp.bfloat16, jnp.float32
    vmem = pl.BlockSpec(memory_space=pltpu.VMEM)
    anywhere = pl.BlockSpec(memory_space=pl.ANY)
    dma = pltpu.SemaphoreType.DMA
    return pl.pallas_call(
        functools.partial(fused_kernel, (rows, cols, width, WINDOW, hidden, heads, group)),
        out_shape=jax.ShapeDtypeStruct((rows, cols), bf16),
        in_specs=[anywhere]
        + [vmem] * 6
        + [pl.BlockSpec(memory_space=pltpu.SMEM), anywhere, vmem]
        + [anywhere] * 6,
        out_specs=vmem,
        scratch_shapes=[
            pltpu.VMEM((rows, cols), bf16),
            pltpu.VMEM(out_weight.shape, bf16),
            pltpu.VMEM((width, 2 * hidden), bf16),
            pltpu.VMEM((width, 2 * hidden), bf16),
            pltpu.VMEM(expert_down.shape[1:], bf16),
            pltpu.VMEM(shared_down.shape, bf16),
            pltpu.VMEM((WINDOW, kv_width), bf16),
            pltpu.VMEM((WINDOW, kv_width), bf16),
            pltpu.VMEM((8, WINDOW), f32),
            pltpu.VMEM((8, WINDOW), f32),
            pltpu.VMEM((WINDOW, rows), f32),
            pltpu.VMEM((rows, WINDOW), f32),
            pltpu.VMEM((rows, heads * HEAD_DIM), bf16),
            pltpu.VMEM((blocks, 2, WINDOW, cols), bf16),
            pltpu.VMEM((blocks, 2, WINDOW, cols), bf16),
            pltpu.VMEM((blocks, WINDOW, cols), bf16),
            pltpu.VMEM((blocks, WINDOW, cols), bf16),
            pltpu.VMEM((rows, cols), f32),
            pltpu.VMEM((4, 4, rows, cols), bf16),
            pltpu.VMEM((rows, width), bf16),
            pltpu.VMEM((5, 4, rows, hidden), bf16),
            pltpu.VMEM((4, rows, cols), bf16),
            pltpu.VMEM((4, rows, cols), bf16),
            pltpu.VMEM((rows, cols), f32),
            dma((8,)),
            dma((3,)),
            dma((3,)),
            dma((blocks, 3)),
            dma((blocks, 3)),
            dma((7, 4, blocks)),
            dma((4, 4, blocks)),
            dma((3, 5)),
            dma((5, 4)),
            dma((4,)),
            dma((4,)),
        ],
        compiler_params=pltpu.CompilerParams(collective_id=0, has_side_effects=True),
    )(
        residual,
        queries,
        keys,
        values,
        segments[None, :],
        routes.T,
        route_weight.T,
        sinks,
        out_weight,
        norm_gain[None, :],
        expert_gate,
        expert_up,
        expert_down,
        shared_gate,
        shared_up,
        shared_down,
    )


def solution(mesh):
    placed = (
        P(("grp", "sp"), None),
        P(("grp", "sp"), "tp"),
        P(("grp", "sp"), "tp"),
        P(("grp", "sp"), "tp"),
        P(("grp", "sp")),
        P(("grp", "sp"), None),
        P(("grp", "sp"), None),
        P("tp"),
        P("tp", None),
        P(),
        P("sp", None, "tp"),
        P("sp", None, "tp"),
        P("sp", None, "tp"),
        P(None, "tp"),
        P(None, "tp"),
        P(None, "tp"),
    )
    return jax.shard_map(
        layer, mesh=mesh, in_specs=placed, out_specs=P(("grp", "sp"), "tp"), check_vma=False
    )
```

```python
import functools
import jax
import jax.numpy as jnp
from jax import lax
from jax.experimental import pallas as pl
from jax.experimental.pallas import tpu as pltpu
from jax.sharding import PartitionSpec as P

HEAD_DIM = 64
WINDOW = 128


epsilon = 1e-06


def passed_along(value, axis, steps):
    count = lax.axis_size(axis)
    leading, last = (max(0, -steps), min(count, count - steps))
    return lax.ppermute(value, axis, [(source, source + steps) for source in range(leading, last)])


def banded(prev_rows, own_rows, window_len):
    blocks = own_rows.shape[0] // window_len
    joined = jnp.concatenate([prev_rows, own_rows], axis=0)
    shaped = joined.reshape((blocks + 1, window_len) + own_rows.shape[1:])
    return jnp.concatenate([shaped[:-1], shaped[1:]], axis=1)


def shards(
    residual,
    queries,
    keys,
    values,
    segments,
    routes,
    route_weight,
    sinks,
    out_weight,
    norm_gain,
    expert_gate,
    expert_up,
    expert_down,
    shared_gate,
    shared_up,
    shared_down,
):
    rows_here = residual.shape[0]
    model_width = residual.shape[1]
    tp_count = lax.axis_size("tp")
    tp_index = lax.axis_index("tp")
    head_local = queries.shape[1] // HEAD_DIM
    kv_local = keys.shape[1] // HEAD_DIM
    group_size = head_local // kv_local
    window_len = WINDOW
    blocks = rows_here // window_len
    own_marks = (segments % 256 + 1).astype(jnp.bfloat16)
    prev_keys, prev_values, prev_marks = passed_along(
        (
            keys[rows_here - window_len :],
            values[rows_here - window_len :],
            own_marks[rows_here - window_len :],
        ),
        "sp",
        1,
    )
    key_band = banded(prev_keys, keys, window_len).reshape(
        blocks, 2 * window_len, kv_local, HEAD_DIM
    )
    value_band = banded(prev_values, values, window_len).reshape(
        blocks, 2 * window_len, kv_local, HEAD_DIM
    )
    mark_band = banded(prev_marks, own_marks, window_len).astype(jnp.float32)
    query_marks = own_marks.reshape(blocks, window_len).astype(jnp.float32)
    query_blocks = queries.reshape(blocks, window_len, kv_local, group_size, HEAD_DIM)
    scores = jnp.einsum(
        "nqhgd,nkhd->nhgqk", query_blocks, key_band, preferred_element_type=jnp.float32
    ) * HEAD_DIM ** (-0.5)
    offsets = jnp.arange(window_len)[:, None] + window_len - jnp.arange(2 * window_len)[None, :]
    allowed = (
        (offsets >= 0) & (offsets < window_len) & (query_marks[:, :, None] == mark_band[:, None, :])
    )
    sink_logits = sinks.reshape(kv_local, group_size)[None, :, :, None]
    masked = jnp.where(allowed[:, None, None], scores, -jnp.inf)
    top_score = jnp.maximum(jnp.max(masked, axis=-1), sink_logits)
    exp_terms = jnp.where(allowed[:, None, None], jnp.exp(scores - top_score[..., None]), 0.0)
    denominator = jnp.sum(exp_terms, axis=-1) + jnp.exp(sink_logits - top_score)
    probabilities = (exp_terms / denominator[..., None]).astype(jnp.bfloat16)
    attended = jnp.einsum(
        "nhgqk,nkhd->nqhgd", probabilities, value_band, preferred_element_type=jnp.float32
    )
    attended = attended.astype(jnp.bfloat16).reshape(rows_here, head_local * HEAD_DIM)
    partial_value = jnp.dot(attended, out_weight, preferred_element_type=jnp.float32)
    col_width = model_width // tp_count
    col_start = tp_index * col_width
    summed = lax.psum(partial_value, "tp")
    updated = (residual.astype(jnp.float32) + summed).astype(jnp.bfloat16)
    updated_f32 = updated.astype(jnp.float32)
    inv_rms = lax.rsqrt(jnp.mean(updated_f32 * updated_f32, axis=-1, keepdims=True) + epsilon)
    normed = (updated_f32 * inv_rms * norm_gain).astype(jnp.bfloat16)
    updated_cols = lax.dynamic_slice_in_dim(updated, col_start, col_width, 1)
    normed_cols = lax.dynamic_slice_in_dim(normed, col_start, col_width, 1)
    shared_pre = jnp.dot(normed, shared_gate, preferred_element_type=jnp.float32)
    shared_lin = jnp.dot(normed, shared_up, preferred_element_type=jnp.float32)
    shared_act = (jax.nn.silu(shared_pre) * shared_lin).astype(jnp.bfloat16)
    top_count = routes.shape[1]
    experts = lax.axis_size("sp")
    capacity = 2 * rows_here * top_count // experts
    flat_ids = routes.reshape(-1)
    one_hot = (flat_ids[:, None] == jnp.arange(experts, dtype=jnp.int32)[None, :]).astype(jnp.int32)
    rank_in = jnp.cumsum(one_hot, axis=0) - one_hot
    slot_dest = flat_ids * capacity + jnp.sum(rank_in * one_hot, axis=1)
    token_of = jnp.arange(rows_here * top_count, dtype=jnp.int32) // top_count
    slot_token = jnp.full((experts * capacity,), -1, jnp.int32).at[slot_dest].set(token_of)
    filled = slot_token >= 0
    safe_token = jnp.where(filled, slot_token, 0)
    outgoing = jnp.where(filled[:, None], normed_cols[safe_token], jnp.zeros((), jnp.bfloat16))
    pieces = lax.all_to_all(
        outgoing.reshape(experts, capacity, col_width),
        "sp",
        split_axis=0,
        concat_axis=0,
        tiled=True,
    )
    arrived = lax.all_gather(pieces, "tp", axis=2, tiled=True)
    expert_rows = arrived.reshape(-1, model_width)
    gate_pre = jnp.dot(expert_rows, expert_gate[0], preferred_element_type=jnp.float32)
    up_lin = jnp.dot(expert_rows, expert_up[0], preferred_element_type=jnp.float32)
    expert_act = (jax.nn.silu(gate_pre) * up_lin).astype(jnp.bfloat16)
    gathered_expert, gathered_shared = (
        lax.all_gather(expert_act, "tp", axis=1, tiled=True),
        lax.all_gather(shared_act, "tp", axis=1, tiled=True),
    )
    expert_out = jnp.dot(
        gathered_expert, expert_down[0], preferred_element_type=jnp.float32
    ).astype(jnp.bfloat16)
    returned = lax.all_to_all(
        expert_out.reshape(experts, capacity, col_width),
        "sp",
        split_axis=0,
        concat_axis=0,
        tiled=True,
    )
    returned = returned.reshape(experts * capacity, col_width)
    picked = returned[slot_dest].astype(jnp.float32).reshape(rows_here, top_count, col_width)
    routed = jnp.sum(picked * route_weight[:, :, None], axis=1)
    shared_cols = jnp.dot(gathered_shared, shared_down, preferred_element_type=jnp.float32)
    return (updated_cols.astype(jnp.float32) + shared_cols + routed).astype(jnp.bfloat16)


MESH = pl.DeviceIdType.MESH
PARTS = 4
ALONG = 1


def fused_kernel(
    dims,
    res_hbm,
    q_ref,
    k_ref,
    v_ref,
    seg_ref,
    routes_ref,
    rw_ref,
    sinks_ref,
    wo_hbm,
    gain_ref,
    eg_hbm,
    eu_hbm,
    ed_hbm,
    sg_hbm,
    su_hbm,
    sd_hbm,
    out_ref,
    res_v,
    wo_v,
    gu_v,
    sgu_v,
    dn_v,
    sdn_v,
    kh,
    vh,
    mh,
    marks_v,
    aux_rows,
    aux_ref,
    att,
    b1s,
    b1r,
    b2s,
    b2r,
    keep,
    upd,
    norm_v,
    act,
    eout,
    eback,
    acc,
    w_sem,
    halo_s,
    halo_r,
    b_s,
    b_r,
    u_s,
    u_r,
    a_s,
    a_r,
    e_s,
    e_r,
):
    rows, cols, width, window, hidden, heads, group = dims
    bf16, f32 = jnp.bfloat16, jnp.float32
    s = lax.axis_index("sp")
    t = lax.axis_index("tp")
    core = t % 2
    chip = t // 2
    mate = t + 1 - 2 * core
    over = t + 2 - 4 * chip
    diag = 3 - t

    def remote(src, dst, send, recv, sp, tp):
        return pltpu.make_async_remote_copy(
            src_ref=src,
            dst_ref=dst,
            send_sem=send,
            recv_sem=recv,
            device_id={"sp": sp, "tp": tp},
            device_id_type=MESH,
        )

    own_cols = pl.ds(pl.multiple_of(t * cols, cols), cols)
    loads = [
        pltpu.make_async_copy(wo_hbm, wo_v, w_sem.at[0]),
        pltpu.make_async_copy(res_hbm.at[:, own_cols], res_v, w_sem.at[1]),
        pltpu.make_async_copy(eg_hbm.at[0], gu_v.at[:, pl.ds(0, hidden)], w_sem.at[2]),
        pltpu.make_async_copy(eu_hbm.at[0], gu_v.at[:, pl.ds(hidden, hidden)], w_sem.at[3]),
        pltpu.make_async_copy(sg_hbm, sgu_v.at[:, pl.ds(0, hidden)], w_sem.at[4]),
        pltpu.make_async_copy(su_hbm, sgu_v.at[:, pl.ds(hidden, hidden)], w_sem.at[5]),
        pltpu.make_async_copy(ed_hbm.at[0], dn_v, w_sem.at[6]),
        pltpu.make_async_copy(sd_hbm, sdn_v, w_sem.at[7]),
    ]
    for load in loads:
        load.start()

    top_count = routes_ref.shape[0]
    aux_rows[...] = jnp.zeros_like(aux_rows)
    aux_rows[0:1, :] = seg_ref[...].astype(f32)
    aux_rows[1 : 1 + top_count, :] = routes_ref[...].astype(f32)
    aux_rows[1 + top_count : 1 + 2 * top_count, :] = rw_ref[...]
    marks_v[...] = jnp.broadcast_to(aux_rows[0:1, pl.ds(rows - window, window)], (8, window))
    barrier = pltpu.get_barrier_semaphore()
    pl.semaphore_signal(barrier, inc=1, device_id={"sp": s, "tp": mate}, device_id_type=MESH)
    pl.semaphore_signal(barrier, inc=1, device_id={"sp": s, "tp": over}, device_id_type=MESH)
    for step in range(1, 4):
        pl.semaphore_signal(
            barrier, inc=1, device_id={"sp": (s + step) % 4, "tp": t}, device_id_type=MESH
        )
    pl.semaphore_wait(barrier, 5)

    def marks_across(n):
        return aux_rows[0:1, pl.ds(n * window, window)]

    tail = pl.ds(rows - window, window)
    up_sp, down_sp = (s + 1) % 4, (s + 3) % 4
    halos = [
        remote(k_ref.at[tail], kh, halo_s.at[0], halo_r.at[0], up_sp, t),
        remote(v_ref.at[tail], vh, halo_s.at[1], halo_r.at[1], up_sp, t),
        remote(marks_v, mh, halo_s.at[2], halo_r.at[2], up_sp, t),
    ]

    @pl.when(s < 3)
    def _():
        for copy in halos:
            copy.start()

    @pl.when(s == 0)
    def _():
        kh[...] = jnp.zeros_like(kh)
        vh[...] = jnp.zeros_like(vh)
        mh[...] = jnp.full(mh.shape, -1.0, f32)

    for n in range(rows // window):
        here = pl.ds(n * window, window)
        aux_ref[here, :] = jnp.transpose(aux_rows[:, here])

    q_pos = lax.broadcasted_iota(jnp.int32, (window, window), 0)
    k_pos = lax.broadcasted_iota(jnp.int32, (window, window), 1)

    def attend(n):
        here = pl.ds(n * window, window)
        if n == 0:
            k_prev, v_prev, m_prev = kh[...], vh[...], mh[0:1, :]
        else:
            before = pl.ds((n - 1) * window, window)
            k_prev, v_prev, m_prev = k_ref[before, :], v_ref[before, :], marks_across(n - 1)
        k_own, v_own, m_own = k_ref[here, :], v_ref[here, :], marks_across(n)
        marks = aux_ref[here, 0:1]
        ok_prev = (k_pos > q_pos) & (marks == m_prev)
        ok_own = (k_pos <= q_pos) & (marks == m_own)
        for h in range(heads):
            kv = slice((h // group) * HEAD_DIM, (h // group + 1) * HEAD_DIM)
            qh = q_ref[here, h * HEAD_DIM : (h + 1) * HEAD_DIM]
            contract = (((1,), (1,)), ((), ()))
            sc_prev = lax.dot_general(
                qh, k_prev[:, kv], contract, preferred_element_type=f32
            ) * HEAD_DIM ** (-0.5)
            sc_own = lax.dot_general(
                qh, k_own[:, kv], contract, preferred_element_type=f32
            ) * HEAD_DIM ** (-0.5)
            sc_prev = jnp.where(ok_prev, sc_prev, -jnp.inf)
            sc_own = jnp.where(ok_own, sc_own, -jnp.inf)
            sink = sinks_ref[h]
            top = jnp.maximum(
                jnp.max(jnp.maximum(sc_prev, sc_own), axis=-1, keepdims=True), sink
            )
            ex_prev = jnp.exp(sc_prev - top)
            ex_own = jnp.exp(sc_own - top)
            total = jnp.sum(ex_prev + ex_own, axis=-1, keepdims=True) + jnp.exp(sink - top)
            inverse = 1.0 / total
            p_prev = (ex_prev * inverse).astype(bf16)
            p_own = (ex_own * inverse).astype(bf16)
            got = jnp.dot(p_prev, v_prev[:, kv], preferred_element_type=f32) + jnp.dot(
                p_own, v_own[:, kv], preferred_element_type=f32
            )
            att[here, h * HEAD_DIM : (h + 1) * HEAD_DIM] = got.astype(bf16)

    def project(n, chunk):
        where = pl.ds(pl.multiple_of(chunk * cols, cols), cols)
        return jnp.dot(
            att[pl.ds(n * window, window), :], wo_v[:, where], preferred_element_type=f32
        )

    halves = list(range(rows // window))[::-1]
    pending = []
    first = {}
    for n in halves:
        if n == 0:

            @pl.when(s > 0)
            def _():
                for copy in halos:
                    copy.wait_recv()

        attend(n)
        if n == halves[0]:
            loads[0].wait()
        for far in (1, 0):
            chunk = (over if far else t) + 1 - 2 * core
            b1s[n, far] = project(n, chunk).astype(bf16)
            copy = remote(
                b1s.at[n, far], b1r.at[n, far], b_s.at[n, far], b_r.at[n, far], s, mate
            )
            copy.start()
            pending.append(copy)
            first[n, far] = copy
    second = {}
    for n in halves:
        mine = project(n, over)
        first[n, 1].wait_recv()
        b2s[n] = (mine + b1r[n, 1].astype(f32)).astype(bf16)
        copy = remote(b2s.at[n], b2r.at[n], b_s.at[n, 2], b_r.at[n, 2], s, over)
        copy.start()
        pending.append(copy)
        second[n] = copy
    loads[1].wait()
    for n in halves:
        here = pl.ds(n * window, window)
        mine = project(n, t) + res_v[here, :].astype(f32)
        first[n, 0].wait_recv()
        keep[here, :] = mine + b1r[n, 0].astype(f32)

    parts = u_s.shape[2]
    part_rows = rows // parts
    per_half = window // part_rows
    listed = [n * per_half + i for n in halves for i in range(per_half)]

    def of_half(n):
        return [p for p in listed if n is None or p // per_half == n]

    def piece(b, chunk, n):
        return upd.at[b, chunk, pl.ds(n * part_rows, part_rows)]

    def share(kind, k, b, chunk, n, sp, tp):
        return remote(
            piece(b, chunk, n),
            piece(b, chunk, n),
            u_s.at[kind, k, n],
            u_r.at[b, chunk, n],
            sp,
            tp,
        )

    conditional = []
    for n in halves:
        here = pl.ds(n * window, window)
        second[n].wait_recv()
        upd[s, t, here, :] = (keep[here, :] + b2r[n].astype(f32)).astype(bf16)
        for p in of_half(n):
            over_copy = share(3, 0, s, t, p, s, over)
            over_copy.start()
            up_copy = share(0, 0, s, t, p, up_sp, t)
            down_copy = share(1, 0, s, t, p, down_sp, t)

            @pl.when(s < 3)
            def _(up_copy=up_copy):
                up_copy.start()

            @pl.when(s > 0)
            def _(down_copy=down_copy):
                down_copy.start()

            mate_copy = share(2, 0, s, t, p, s, mate)
            mate_copy.start()
            pending += [over_copy, mate_copy]
            conditional += [(s < 3, up_copy), (s > 0, down_copy)]

    side = s // 2
    edge = s + side * (3 - 2 * s)
    order = [s]
    for k in range(1, 4):
        flat = (k, k + edge, k - 2 * edge, k)[k]
        order.append(flat + side * (3 - 2 * flat))

    along = listed[:ALONG]

    def onward(k, kinds, chunk, n):
        b = order[k]
        to_up = share(kinds[0], k, b, chunk, n, up_sp, t)
        to_down = share(kinds[1], k, b, chunk, n, down_sp, t)
        rising = s < 3 if k == 0 else (b < s) & (s < 3)
        falling = s > 0 if k == 0 else (b > s) & (s > 0)

        @pl.when(rising)
        def _():
            to_up.start()

        @pl.when(falling)
        def _():
            to_down.start()

        conditional.extend([(rising, to_up), (falling, to_down)])

    def arrive(k, half=None):
        b = order[k]
        for n in of_half(half):
            share(0, k, b, t, n, s, mate).wait_recv()
            onward(k, (0, 1), t, n)
            if n not in along:
                copy = share(3, k, b, t, n, s, over)
                copy.start()
                pending.append(copy)
            mate_copy = share(2, k, b, t, n, s, mate)
            mate_copy.start()
            pending.append(mate_copy)

    def relay_half(k, n):
        b = order[k]
        share(4, k, b, over, n, s, mate).wait_recv()
        if n in along:
            onward(k, (5, 6), over, n)
        copy = share(4, k, b, over, n, s, mate)
        copy.start()
        pending.append(copy)

    def relay(k, half=None):
        for n in of_half(half):
            if k == 0 or n not in along:
                relay_half(k, n)

    def arrive_over(k):
        for n in along:
            relay_half(k, n)

    def normalize(k, half):
        b = order[k]
        for n in of_half(half):
            share(2, k, b, mate, n, s, mate).wait_recv()
            share(4, k, b, diag, n, s, mate).wait_recv()
        step = 32

        def body(i, carry):
            here = pl.ds(pl.multiple_of(half * window + i * step, step), step)
            squares = jnp.zeros((step, 1), f32)
            for chunk in range(4):
                part = upd[b, chunk, here, :].astype(f32)
                squares = squares + jnp.sum(part * part, axis=-1, keepdims=True)
            inv = lax.rsqrt(squares / width + epsilon)
            for chunk in range(4):
                part = upd[b, chunk, here, :].astype(f32)
                span = slice(chunk * cols, (chunk + 1) * cols)
                norm_v[here, span] = (part * inv * gain_ref[0:1, span]).astype(bf16)
            return carry

        lax.fori_loop(0, window // step, body, 0)

    def pass_on(slot, kind, chunk, tp, half):
        place = act.at[slot, chunk, pl.ds(half * window, window)]
        return remote(
            place, place, a_s.at[kind, slot, half], a_r.at[slot, chunk, half], s, tp
        )

    def activate(slot, weight, half):
        here = pl.ds(half * window, window)
        both = jnp.dot(norm_v[here, :], weight[...], preferred_element_type=f32)
        gate, lin = both[:, :hidden], both[:, hidden:]
        act[slot, t, here, :] = (gate / (1.0 + jnp.exp(-gate)) * lin).astype(bf16)
        for kind, tp in ((0, over), (1, mate)):
            copy = pass_on(slot, kind, t, tp, half)
            copy.start()
            pending.append(copy)

    def relay_act(slot, half):
        pass_on(slot, 2, over, mate, half).wait_recv()
        copy = pass_on(slot, 2, over, mate, half)
        copy.start()
        pending.append(copy)

    def contract_act(slot, weight, half):
        pass_on(slot, 1, mate, mate, half).wait_recv()
        pass_on(slot, 2, diag, mate, half).wait_recv()
        total = None
        for chunk in range(4):
            part = jnp.dot(
                act[slot, chunk, pl.ds(half * window, window), :],
                weight[chunk * hidden : (chunk + 1) * hidden, :],
                preferred_element_type=f32,
            )
            total = part if total is None else total + part
        return total

    def give_back(k, b, half):
        here = pl.ds(half * window, window)
        return remote(
            eout.at[k, here], eback.at[b, here], e_s.at[k, half], e_r.at[b, half], order[k], t
        )

    def finish(k, half):
        here = pl.ds(half * window, window)
        eout[k, here, :] = contract_act(k, dn_v, half).astype(bf16)
        copy = give_back(k, s, half)
        copy.start()
        pending.append(copy)

    def expert(k, half):
        normalize(k, half)
        activate(k, gu_v, half)

    def each(step, *given):
        for n in halves:
            step(*given, n)

    early, late = halves[0], halves[-1]
    arrive(1)
    relay(0)
    arrive(2)
    arrive_over(1)
    relay(1)
    loads[2].wait()
    loads[3].wait()
    each(expert, 1)
    arrive(3, early)
    arrive_over(2)
    each(expert, 0)
    loads[4].wait()
    loads[5].wait()
    each(activate, 4, sgu_v)
    relay(2)
    each(expert, 2)
    each(relay_act, 1)
    loads[6].wait()
    each(finish, 1)
    arrive(3, late)
    arrive_over(3)
    each(relay_act, 0)
    each(relay_act, 4)
    relay(3, early)
    expert(3, early)
    each(relay_act, 2)
    each(finish, 2)
    relay(3, late)
    expert(3, late)
    for n in halves:
        eout[0, pl.ds(n * window, window), :] = contract_act(0, dn_v, n).astype(bf16)
    relay_act(3, early)
    finish(3, early)
    loads[7].wait()
    for n in halves:
        here = pl.ds(n * window, window)
        acc[here, :] = contract_act(4, sdn_v, n)
    relay_act(3, late)
    finish(3, late)

    def weight_of(e):
        total = jnp.zeros((rows, 1), f32)
        for k in range(1, top_count + 1):
            weight = aux_ref[:, top_count + k : top_count + k + 1]
            named = aux_ref[:, k : k + 1] == jnp.full((rows, 1), e, jnp.int32).astype(f32)
            total = total + jnp.where(named, weight, 0.0)
        return total

    weights = [weight_of(order[k]) for k in range(4)]
    for n in halves:
        here = pl.ds(n * window, window)
        acc[here, :] = (
            acc[here, :]
            + upd[s, t, here, :].astype(f32)
            + weights[0][n * window : (n + 1) * window] * eout[0, here, :].astype(f32)
        )
    for k in range(1, 4):
        for n in halves:
            here = pl.ds(n * window, window)
            give_back(k, order[k], n).wait_recv()
            more = weights[k][n * window : (n + 1) * window] * eback[order[k], here, :].astype(f32)
            if k < 3:
                acc[here, :] = acc[here, :] + more
            else:
                out_ref[here, :] = (acc[here, :] + more).astype(bf16)

    for copy in pending:
        copy.wait_send()
    for when, copy in conditional:

        @pl.when(when)
        def _():
            copy.wait_send()

    @pl.when(s < 3)
    def _():
        for copy in halos:
            copy.wait_send()


def layer(
    residual,
    queries,
    keys,
    values,
    segments,
    routes,
    route_weight,
    sinks,
    out_weight,
    norm_gain,
    expert_gate,
    expert_up,
    expert_down,
    shared_gate,
    shared_up,
    shared_down,
):
    arguments = (
        residual,
        queries,
        keys,
        values,
        segments,
        routes,
        route_weight,
        sinks,
        out_weight,
        norm_gain,
        expert_gate,
        expert_up,
        expert_down,
        shared_gate,
        shared_up,
        shared_down,
    )
    rows, width = residual.shape
    n_sp, n_tp = lax.axis_size("sp"), lax.axis_size("tp")
    capacity = 2 * rows * routes.shape[1] // n_sp
    hidden = expert_gate.shape[2]
    if n_sp != 4 or n_tp != 4 or capacity < rows or shared_gate.shape[1] != hidden:
        return shards(*arguments)
    cols = width // n_tp
    heads = queries.shape[1] // HEAD_DIM
    group = queries.shape[1] // keys.shape[1]
    kv_width = keys.shape[1]
    blocks = rows // WINDOW
    bf16, f32 = jnp.bfloat16, jnp.float32
    vmem = pl.BlockSpec(memory_space=pltpu.VMEM)
    anywhere = pl.BlockSpec(memory_space=pl.ANY)
    dma = pltpu.SemaphoreType.DMA
    return pl.pallas_call(
        functools.partial(fused_kernel, (rows, cols, width, WINDOW, hidden, heads, group)),
        out_shape=jax.ShapeDtypeStruct((rows, cols), bf16),
        in_specs=[anywhere]
        + [vmem] * 6
        + [pl.BlockSpec(memory_space=pltpu.SMEM), anywhere, vmem]
        + [anywhere] * 6,
        out_specs=vmem,
        scratch_shapes=[
            pltpu.VMEM((rows, cols), bf16),
            pltpu.VMEM(out_weight.shape, bf16),
            pltpu.VMEM((width, 2 * hidden), bf16),
            pltpu.VMEM((width, 2 * hidden), bf16),
            pltpu.VMEM(expert_down.shape[1:], bf16),
            pltpu.VMEM(shared_down.shape, bf16),
            pltpu.VMEM((WINDOW, kv_width), bf16),
            pltpu.VMEM((WINDOW, kv_width), bf16),
            pltpu.VMEM((8, WINDOW), f32),
            pltpu.VMEM((8, WINDOW), f32),
            pltpu.VMEM((WINDOW, rows), f32),
            pltpu.VMEM((rows, WINDOW), f32),
            pltpu.VMEM((rows, heads * HEAD_DIM), bf16),
            pltpu.VMEM((blocks, 2, WINDOW, cols), bf16),
            pltpu.VMEM((blocks, 2, WINDOW, cols), bf16),
            pltpu.VMEM((blocks, WINDOW, cols), bf16),
            pltpu.VMEM((blocks, WINDOW, cols), bf16),
            pltpu.VMEM((rows, cols), f32),
            pltpu.VMEM((4, 4, rows, cols), bf16),
            pltpu.VMEM((rows, width), bf16),
            pltpu.VMEM((5, 4, rows, hidden), bf16),
            pltpu.VMEM((4, rows, cols), bf16),
            pltpu.VMEM((4, rows, cols), bf16),
            pltpu.VMEM((rows, cols), f32),
            dma((8,)),
            dma((3,)),
            dma((3,)),
            dma((blocks, 3)),
            dma((blocks, 3)),
            dma((7, 4, PARTS)),
            dma((4, 4, PARTS)),
            dma((3, 5, blocks)),
            dma((5, 4, blocks)),
            dma((4, blocks)),
            dma((4, blocks)),
        ],
        compiler_params=pltpu.CompilerParams(collective_id=0, has_side_effects=True),
    )(
        residual,
        queries,
        keys,
        values,
        segments[None, :],
        routes.T,
        route_weight.T,
        sinks,
        out_weight,
        norm_gain[None, :],
        expert_gate,
        expert_up,
        expert_down,
        shared_gate,
        shared_up,
        shared_down,
    )


def solution(mesh):
    placed = (
        P(("grp", "sp"), None),
        P(("grp", "sp"), "tp"),
        P(("grp", "sp"), "tp"),
        P(("grp", "sp"), "tp"),
        P(("grp", "sp")),
        P(("grp", "sp"), None),
        P(("grp", "sp"), None),
        P("tp"),
        P("tp", None),
        P(),
        P("sp", None, "tp"),
        P("sp", None, "tp"),
        P("sp", None, "tp"),
        P(None, "tp"),
        P(None, "tp"),
        P(None, "tp"),
    )
    return jax.shard_map(
        layer, mesh=mesh, in_specs=placed, out_specs=P(("grp", "sp"), "tp"), check_vma=False
    )
```

```python
import functools
import jax
import jax.numpy as jnp
from jax import lax
from jax.experimental import pallas as pl
from jax.experimental.pallas import tpu as pltpu
from jax.sharding import PartitionSpec as P

HEAD_DIM = 64
WINDOW = 128


epsilon = 1e-06


def passed_along(value, axis, steps):
    count = lax.axis_size(axis)
    leading, last = (max(0, -steps), min(count, count - steps))
    return lax.ppermute(value, axis, [(source, source + steps) for source in range(leading, last)])


def banded(prev_rows, own_rows, window_len):
    blocks = own_rows.shape[0] // window_len
    joined = jnp.concatenate([prev_rows, own_rows], axis=0)
    shaped = joined.reshape((blocks + 1, window_len) + own_rows.shape[1:])
    return jnp.concatenate([shaped[:-1], shaped[1:]], axis=1)


def shards(
    residual,
    queries,
    keys,
    values,
    segments,
    routes,
    route_weight,
    sinks,
    out_weight,
    norm_gain,
    expert_gate,
    expert_up,
    expert_down,
    shared_gate,
    shared_up,
    shared_down,
):
    rows_here = residual.shape[0]
    model_width = residual.shape[1]
    tp_count = lax.axis_size("tp")
    tp_index = lax.axis_index("tp")
    head_local = queries.shape[1] // HEAD_DIM
    kv_local = keys.shape[1] // HEAD_DIM
    group_size = head_local // kv_local
    window_len = WINDOW
    blocks = rows_here // window_len
    own_marks = (segments % 256 + 1).astype(jnp.bfloat16)
    prev_keys, prev_values, prev_marks = passed_along(
        (
            keys[rows_here - window_len :],
            values[rows_here - window_len :],
            own_marks[rows_here - window_len :],
        ),
        "sp",
        1,
    )
    key_band = banded(prev_keys, keys, window_len).reshape(
        blocks, 2 * window_len, kv_local, HEAD_DIM
    )
    value_band = banded(prev_values, values, window_len).reshape(
        blocks, 2 * window_len, kv_local, HEAD_DIM
    )
    mark_band = banded(prev_marks, own_marks, window_len).astype(jnp.float32)
    query_marks = own_marks.reshape(blocks, window_len).astype(jnp.float32)
    query_blocks = queries.reshape(blocks, window_len, kv_local, group_size, HEAD_DIM)
    scores = jnp.einsum(
        "nqhgd,nkhd->nhgqk", query_blocks, key_band, preferred_element_type=jnp.float32
    ) * HEAD_DIM ** (-0.5)
    offsets = jnp.arange(window_len)[:, None] + window_len - jnp.arange(2 * window_len)[None, :]
    allowed = (
        (offsets >= 0) & (offsets < window_len) & (query_marks[:, :, None] == mark_band[:, None, :])
    )
    sink_logits = sinks.reshape(kv_local, group_size)[None, :, :, None]
    masked = jnp.where(allowed[:, None, None], scores, -jnp.inf)
    top_score = jnp.maximum(jnp.max(masked, axis=-1), sink_logits)
    exp_terms = jnp.where(allowed[:, None, None], jnp.exp(scores - top_score[..., None]), 0.0)
    denominator = jnp.sum(exp_terms, axis=-1) + jnp.exp(sink_logits - top_score)
    probabilities = (exp_terms / denominator[..., None]).astype(jnp.bfloat16)
    attended = jnp.einsum(
        "nhgqk,nkhd->nqhgd", probabilities, value_band, preferred_element_type=jnp.float32
    )
    attended = attended.astype(jnp.bfloat16).reshape(rows_here, head_local * HEAD_DIM)
    partial_value = jnp.dot(attended, out_weight, preferred_element_type=jnp.float32)
    col_width = model_width // tp_count
    col_start = tp_index * col_width
    summed = lax.psum(partial_value, "tp")
    updated = (residual.astype(jnp.float32) + summed).astype(jnp.bfloat16)
    updated_f32 = updated.astype(jnp.float32)
    inv_rms = lax.rsqrt(jnp.mean(updated_f32 * updated_f32, axis=-1, keepdims=True) + epsilon)
    normed = (updated_f32 * inv_rms * norm_gain).astype(jnp.bfloat16)
    updated_cols = lax.dynamic_slice_in_dim(updated, col_start, col_width, 1)
    normed_cols = lax.dynamic_slice_in_dim(normed, col_start, col_width, 1)
    shared_pre = jnp.dot(normed, shared_gate, preferred_element_type=jnp.float32)
    shared_lin = jnp.dot(normed, shared_up, preferred_element_type=jnp.float32)
    shared_act = (jax.nn.silu(shared_pre) * shared_lin).astype(jnp.bfloat16)
    top_count = routes.shape[1]
    experts = lax.axis_size("sp")
    capacity = 2 * rows_here * top_count // experts
    flat_ids = routes.reshape(-1)
    one_hot = (flat_ids[:, None] == jnp.arange(experts, dtype=jnp.int32)[None, :]).astype(jnp.int32)
    rank_in = jnp.cumsum(one_hot, axis=0) - one_hot
    slot_dest = flat_ids * capacity + jnp.sum(rank_in * one_hot, axis=1)
    token_of = jnp.arange(rows_here * top_count, dtype=jnp.int32) // top_count
    slot_token = jnp.full((experts * capacity,), -1, jnp.int32).at[slot_dest].set(token_of)
    filled = slot_token >= 0
    safe_token = jnp.where(filled, slot_token, 0)
    outgoing = jnp.where(filled[:, None], normed_cols[safe_token], jnp.zeros((), jnp.bfloat16))
    pieces = lax.all_to_all(
        outgoing.reshape(experts, capacity, col_width),
        "sp",
        split_axis=0,
        concat_axis=0,
        tiled=True,
    )
    arrived = lax.all_gather(pieces, "tp", axis=2, tiled=True)
    expert_rows = arrived.reshape(-1, model_width)
    gate_pre = jnp.dot(expert_rows, expert_gate[0], preferred_element_type=jnp.float32)
    up_lin = jnp.dot(expert_rows, expert_up[0], preferred_element_type=jnp.float32)
    expert_act = (jax.nn.silu(gate_pre) * up_lin).astype(jnp.bfloat16)
    gathered_expert, gathered_shared = (
        lax.all_gather(expert_act, "tp", axis=1, tiled=True),
        lax.all_gather(shared_act, "tp", axis=1, tiled=True),
    )
    expert_out = jnp.dot(
        gathered_expert, expert_down[0], preferred_element_type=jnp.float32
    ).astype(jnp.bfloat16)
    returned = lax.all_to_all(
        expert_out.reshape(experts, capacity, col_width),
        "sp",
        split_axis=0,
        concat_axis=0,
        tiled=True,
    )
    returned = returned.reshape(experts * capacity, col_width)
    picked = returned[slot_dest].astype(jnp.float32).reshape(rows_here, top_count, col_width)
    routed = jnp.sum(picked * route_weight[:, :, None], axis=1)
    shared_cols = jnp.dot(gathered_shared, shared_down, preferred_element_type=jnp.float32)
    return (updated_cols.astype(jnp.float32) + shared_cols + routed).astype(jnp.bfloat16)


MESH = pl.DeviceIdType.MESH
PARTS = 4
ALONG = 1


def fused_kernel(
    dims,
    res_hbm,
    q_ref,
    k_ref,
    v_ref,
    seg_ref,
    routes_ref,
    rw_ref,
    sinks_ref,
    wo_hbm,
    gain_ref,
    eg_hbm,
    eu_hbm,
    ed_hbm,
    sg_hbm,
    su_hbm,
    sd_hbm,
    out_ref,
    res_v,
    wo_v,
    gu_v,
    sgu_v,
    dn_v,
    sdn_v,
    kh,
    vh,
    mh,
    marks_v,
    aux_rows,
    aux_ref,
    att,
    b1s,
    b1r,
    b2s,
    b2r,
    keep,
    upd,
    norm_v,
    act,
    eout,
    eback,
    acc,
    w_sem,
    halo_s,
    halo_r,
    b_s,
    b_r,
    u_s,
    u_r,
    a_s,
    a_r,
    e_s,
    e_r,
):
    rows, cols, width, window, hidden, heads, group = dims
    bf16, f32 = jnp.bfloat16, jnp.float32
    s = lax.axis_index("sp")
    t = lax.axis_index("tp")
    core = t % 2
    chip = t // 2
    mate = t + 1 - 2 * core
    over = t + 2 - 4 * chip
    diag = 3 - t

    def remote(src, dst, send, recv, sp, tp):
        return pltpu.make_async_remote_copy(
            src_ref=src,
            dst_ref=dst,
            send_sem=send,
            recv_sem=recv,
            device_id={"sp": sp, "tp": tp},
            device_id_type=MESH,
        )

    own_cols = pl.ds(pl.multiple_of(t * cols, cols), cols)
    loads = [
        pltpu.make_async_copy(wo_hbm, wo_v, w_sem.at[0]),
        pltpu.make_async_copy(res_hbm.at[:, own_cols], res_v, w_sem.at[1]),
        pltpu.make_async_copy(eg_hbm.at[0], gu_v.at[:, pl.ds(0, hidden)], w_sem.at[2]),
        pltpu.make_async_copy(eu_hbm.at[0], gu_v.at[:, pl.ds(hidden, hidden)], w_sem.at[3]),
        pltpu.make_async_copy(sg_hbm, sgu_v.at[:, pl.ds(0, hidden)], w_sem.at[4]),
        pltpu.make_async_copy(su_hbm, sgu_v.at[:, pl.ds(hidden, hidden)], w_sem.at[5]),
        pltpu.make_async_copy(ed_hbm.at[0], dn_v, w_sem.at[6]),
        pltpu.make_async_copy(sd_hbm, sdn_v, w_sem.at[7]),
    ]
    for load in loads[:2]:
        load.start()

    top_count = routes_ref.shape[0]
    aux_rows[...] = jnp.zeros_like(aux_rows)
    aux_rows[0:1, :] = seg_ref[...].astype(f32)
    aux_rows[1 : 1 + top_count, :] = routes_ref[...].astype(f32)
    aux_rows[1 + top_count : 1 + 2 * top_count, :] = rw_ref[...]
    marks_v[...] = jnp.broadcast_to(aux_rows[0:1, pl.ds(rows - window, window)], (8, window))
    barrier = pltpu.get_barrier_semaphore()
    pl.semaphore_signal(barrier, inc=1, device_id={"sp": s, "tp": mate}, device_id_type=MESH)
    pl.semaphore_signal(barrier, inc=1, device_id={"sp": s, "tp": over}, device_id_type=MESH)
    for step in range(1, 4):
        pl.semaphore_signal(
            barrier, inc=1, device_id={"sp": (s + step) % 4, "tp": t}, device_id_type=MESH
        )
    pl.semaphore_wait(barrier, 5)

    def marks_across(n):
        return aux_rows[0:1, pl.ds(n * window, window)]

    tail = pl.ds(rows - window, window)
    up_sp, down_sp = (s + 1) % 4, (s + 3) % 4
    halos = [
        remote(k_ref.at[tail], kh, halo_s.at[0], halo_r.at[0], up_sp, t),
        remote(v_ref.at[tail], vh, halo_s.at[1], halo_r.at[1], up_sp, t),
        remote(marks_v, mh, halo_s.at[2], halo_r.at[2], up_sp, t),
    ]

    @pl.when(s < 3)
    def _():
        for copy in halos:
            copy.start()

    @pl.when(s == 0)
    def _():
        kh[...] = jnp.zeros_like(kh)
        vh[...] = jnp.zeros_like(vh)
        mh[...] = jnp.full(mh.shape, -1.0, f32)

    for n in range(rows // window):
        here = pl.ds(n * window, window)
        aux_ref[here, :] = jnp.transpose(aux_rows[:, here])

    q_pos = lax.broadcasted_iota(jnp.int32, (window, window), 0)
    k_pos = lax.broadcasted_iota(jnp.int32, (window, window), 1)

    def attend(n):
        here = pl.ds(n * window, window)
        if n == 0:
            k_prev, v_prev, m_prev = kh[...], vh[...], mh[0:1, :]
        else:
            before = pl.ds((n - 1) * window, window)
            k_prev, v_prev, m_prev = k_ref[before, :], v_ref[before, :], marks_across(n - 1)
        k_own, v_own, m_own = k_ref[here, :], v_ref[here, :], marks_across(n)
        marks = aux_ref[here, 0:1]
        ok_prev = (k_pos > q_pos) & (marks == m_prev)
        ok_own = (k_pos <= q_pos) & (marks == m_own)
        for h in range(heads):
            kv = slice((h // group) * HEAD_DIM, (h // group + 1) * HEAD_DIM)
            qh = q_ref[here, h * HEAD_DIM : (h + 1) * HEAD_DIM]
            contract = (((1,), (1,)), ((), ()))
            sc_prev = lax.dot_general(
                qh, k_prev[:, kv], contract, preferred_element_type=f32
            ) * HEAD_DIM ** (-0.5)
            sc_own = lax.dot_general(
                qh, k_own[:, kv], contract, preferred_element_type=f32
            ) * HEAD_DIM ** (-0.5)
            sc_prev = jnp.where(ok_prev, sc_prev, -jnp.inf)
            sc_own = jnp.where(ok_own, sc_own, -jnp.inf)
            sink = sinks_ref[h]
            top = jnp.maximum(
                jnp.max(jnp.maximum(sc_prev, sc_own), axis=-1, keepdims=True), sink
            )
            ex_prev = jnp.exp(sc_prev - top)
            ex_own = jnp.exp(sc_own - top)
            total = jnp.sum(ex_prev + ex_own, axis=-1, keepdims=True) + jnp.exp(sink - top)
            inverse = 1.0 / total
            p_prev = (ex_prev * inverse).astype(bf16)
            p_own = (ex_own * inverse).astype(bf16)
            got = jnp.dot(p_prev, v_prev[:, kv], preferred_element_type=f32) + jnp.dot(
                p_own, v_own[:, kv], preferred_element_type=f32
            )
            att[here, h * HEAD_DIM : (h + 1) * HEAD_DIM] = got.astype(bf16)

    def project(n, chunk):
        where = pl.ds(pl.multiple_of(chunk * cols, cols), cols)
        return jnp.dot(
            att[pl.ds(n * window, window), :], wo_v[:, where], preferred_element_type=f32
        )

    halves = list(range(rows // window))[::-1]
    pending = []
    first = {}
    second = {}
    for n in halves:
        if n == 0:

            @pl.when(s > 0)
            def _():
                for copy in halos:
                    copy.wait_recv()

        attend(n)
        if n == halves[0]:
            loads[0].wait()
            for load in loads[2:]:
                load.start()
        for far in (1, 0):
            chunk = (over if far else t) + 1 - 2 * core
            b1s[n, far] = project(n, chunk).astype(bf16)
            copy = remote(
                b1s.at[n, far], b1r.at[n, far], b_s.at[n, far], b_r.at[n, far], s, mate
            )
            copy.start()
            pending.append(copy)
            first[n, far] = copy
        mine = project(n, over)
        first[n, 1].wait_recv()
        b2s[n] = (mine + b1r[n, 1].astype(f32)).astype(bf16)
        copy = remote(b2s.at[n], b2r.at[n], b_s.at[n, 2], b_r.at[n, 2], s, over)
        copy.start()
        pending.append(copy)
        second[n] = copy
    loads[1].wait()
    for n in halves:
        here = pl.ds(n * window, window)
        mine = project(n, t) + res_v[here, :].astype(f32)
        first[n, 0].wait_recv()
        keep[here, :] = mine + b1r[n, 0].astype(f32)

    parts = u_s.shape[2]
    part_rows = rows // parts
    per_half = window // part_rows
    listed = [n * per_half + i for n in halves for i in range(per_half)]

    def of_half(n):
        return [p for p in listed if n is None or p // per_half == n]

    def piece(b, chunk, n):
        return upd.at[b, chunk, pl.ds(n * part_rows, part_rows)]

    def share(kind, k, b, chunk, n, sp, tp):
        return remote(
            piece(b, chunk, n),
            piece(b, chunk, n),
            u_s.at[kind, k, n],
            u_r.at[b, chunk, n],
            sp,
            tp,
        )

    conditional = []
    for n in halves:
        here = pl.ds(n * window, window)
        second[n].wait_recv()
        upd[s, t, here, :] = (keep[here, :] + b2r[n].astype(f32)).astype(bf16)
        for p in of_half(n):
            over_copy = share(3, 0, s, t, p, s, over)
            over_copy.start()
            up_copy = share(0, 0, s, t, p, up_sp, t)
            down_copy = share(1, 0, s, t, p, down_sp, t)

            @pl.when(s < 3)
            def _(up_copy=up_copy):
                up_copy.start()

            @pl.when(s > 0)
            def _(down_copy=down_copy):
                down_copy.start()

            mate_copy = share(2, 0, s, t, p, s, mate)
            mate_copy.start()
            pending += [over_copy, mate_copy]
            conditional += [(s < 3, up_copy), (s > 0, down_copy)]

    side = s // 2
    edge = s + side * (3 - 2 * s)
    order = [s]
    for k in range(1, 4):
        flat = (k, k + edge, k - 2 * edge, k)[k]
        order.append(flat + side * (3 - 2 * flat))

    along = listed[:ALONG]

    def onward(k, kinds, chunk, n):
        b = order[k]
        to_up = share(kinds[0], k, b, chunk, n, up_sp, t)
        to_down = share(kinds[1], k, b, chunk, n, down_sp, t)
        rising = s < 3 if k == 0 else (b < s) & (s < 3)
        falling = s > 0 if k == 0 else (b > s) & (s > 0)

        @pl.when(rising)
        def _():
            to_up.start()

        @pl.when(falling)
        def _():
            to_down.start()

        conditional.extend([(rising, to_up), (falling, to_down)])

    def arrive(k, half=None):
        b = order[k]
        for n in of_half(half):
            share(0, k, b, t, n, s, mate).wait_recv()
            onward(k, (0, 1), t, n)
            if n not in along:
                copy = share(3, k, b, t, n, s, over)
                copy.start()
                pending.append(copy)
            mate_copy = share(2, k, b, t, n, s, mate)
            mate_copy.start()
            pending.append(mate_copy)

    def relay_half(k, n):
        b = order[k]
        share(4, k, b, over, n, s, mate).wait_recv()
        if n in along:
            onward(k, (5, 6), over, n)
        copy = share(4, k, b, over, n, s, mate)
        copy.start()
        pending.append(copy)

    def relay(k, half=None):
        for n in of_half(half):
            if k == 0 or n not in along:
                relay_half(k, n)

    def arrive_over(k):
        for n in along:
            relay_half(k, n)

    def span_of(half):
        if half is None:
            return halves, 0, rows
        return [half], half * window, window

    def normalize(k, half=None):
        b = order[k]
        _, begin, length = span_of(half)
        for n in of_half(half):
            share(2, k, b, mate, n, s, mate).wait_recv()
            share(4, k, b, diag, n, s, mate).wait_recv()
        step = 32

        def body(i, carry):
            here = pl.ds(pl.multiple_of(begin + i * step, step), step)
            squares = jnp.zeros((step, 1), f32)
            for chunk in range(4):
                part = upd[b, chunk, here, :].astype(f32)
                squares = squares + jnp.sum(part * part, axis=-1, keepdims=True)
            inv = lax.rsqrt(squares / width + epsilon)
            for chunk in range(4):
                part = upd[b, chunk, here, :].astype(f32)
                span = slice(chunk * cols, (chunk + 1) * cols)
                norm_v[here, span] = (part * inv * gain_ref[0:1, span]).astype(bf16)
            return carry

        lax.fori_loop(0, length // step, body, 0)

    def pass_on(slot, kind, chunk, tp, half):
        place = act.at[slot, chunk, pl.ds(half * window, window)]
        return remote(
            place, place, a_s.at[kind, slot, half], a_r.at[slot, chunk, half], s, tp
        )

    def activate(slot, weight, half=None):
        _, begin, length = span_of(half)
        here = pl.ds(begin, length)
        both = jnp.dot(norm_v[here, :], weight[...], preferred_element_type=f32)
        gate, lin = both[:, :hidden], both[:, hidden:]
        act[slot, t, here, :] = (gate / (1.0 + jnp.exp(-gate)) * lin).astype(bf16)

    def ship(slot, half=None):
        for n in span_of(half)[0]:
            for kind, tp in ((0, over), (1, mate)):
                copy = pass_on(slot, kind, t, tp, n)
                copy.start()
                pending.append(copy)

    def relay_act(slot, half=None):
        for n in span_of(half)[0]:
            pass_on(slot, 2, over, mate, n).wait_recv()
            copy = pass_on(slot, 2, over, mate, n)
            copy.start()
            pending.append(copy)

    def contract_act(slot, weight, half=None):
        listing, begin, length = span_of(half)
        for n in listing:
            pass_on(slot, 1, mate, mate, n).wait_recv()
            pass_on(slot, 2, diag, mate, n).wait_recv()
        total = None
        for chunk in range(4):
            part = jnp.dot(
                act[slot, chunk, pl.ds(begin, length), :],
                weight[chunk * hidden : (chunk + 1) * hidden, :],
                preferred_element_type=f32,
            )
            total = part if total is None else total + part
        return total

    def give_back(k, b, half):
        here = pl.ds(half * window, window)
        return remote(
            eout.at[k, here], eback.at[b, here], e_s.at[k, half], e_r.at[b, half], order[k], t
        )

    def finish(k, half=None):
        listing, begin, length = span_of(half)
        eout[k, pl.ds(begin, length), :] = contract_act(k, dn_v, half).astype(bf16)
        for n in listing:
            copy = give_back(k, s, n)
            copy.start()
            pending.append(copy)

    def expert(k, half=None):
        normalize(k, half)
        activate(k, gu_v, half)
        ship(k, half)

    early, late = halves[0], halves[-1]
    arrive(1)
    relay(0)
    arrive(2)
    arrive_over(1)
    relay(1)
    loads[2].wait()
    loads[3].wait()
    expert(1)
    arrive(3, early)
    arrive_over(2)
    normalize(0)
    activate(0, gu_v)
    relay(2)
    loads[4].wait()
    loads[5].wait()
    activate(4, sgu_v)
    expert(2)
    relay_act(1)
    loads[6].wait()
    finish(1)
    arrive(3, late)
    arrive_over(3)
    relay(3, early)
    expert(3, early)
    relay_act(2)
    finish(2)
    relay(3, late)
    expert(3, late)
    ship(0)
    ship(4)
    relay_act(3, early)
    finish(3, early)
    relay_act(3, late)
    finish(3, late)
    relay_act(0)
    relay_act(4)
    eout[0] = contract_act(0, dn_v).astype(bf16)
    loads[7].wait()
    acc[...] = contract_act(4, sdn_v)

    def weight_of(e):
        total = jnp.zeros((rows, 1), f32)
        for k in range(1, top_count + 1):
            weight = aux_ref[:, top_count + k : top_count + k + 1]
            named = aux_ref[:, k : k + 1] == jnp.full((rows, 1), e, jnp.int32).astype(f32)
            total = total + jnp.where(named, weight, 0.0)
        return total

    weights = [weight_of(order[k]) for k in range(4)]
    for n in halves:
        here = pl.ds(n * window, window)
        acc[here, :] = (
            acc[here, :]
            + upd[s, t, here, :].astype(f32)
            + weights[0][n * window : (n + 1) * window] * eout[0, here, :].astype(f32)
        )
    for k in range(1, 4):
        for n in halves:
            here = pl.ds(n * window, window)
            give_back(k, order[k], n).wait_recv()
            more = weights[k][n * window : (n + 1) * window] * eback[order[k], here, :].astype(f32)
            if k < 3:
                acc[here, :] = acc[here, :] + more
            else:
                out_ref[here, :] = (acc[here, :] + more).astype(bf16)

    for copy in pending:
        copy.wait_send()
    for when, copy in conditional:

        @pl.when(when)
        def _():
            copy.wait_send()

    @pl.when(s < 3)
    def _():
        for copy in halos:
            copy.wait_send()


def layer(
    residual,
    queries,
    keys,
    values,
    segments,
    routes,
    route_weight,
    sinks,
    out_weight,
    norm_gain,
    expert_gate,
    expert_up,
    expert_down,
    shared_gate,
    shared_up,
    shared_down,
):
    arguments = (
        residual,
        queries,
        keys,
        values,
        segments,
        routes,
        route_weight,
        sinks,
        out_weight,
        norm_gain,
        expert_gate,
        expert_up,
        expert_down,
        shared_gate,
        shared_up,
        shared_down,
    )
    rows, width = residual.shape
    n_sp, n_tp = lax.axis_size("sp"), lax.axis_size("tp")
    capacity = 2 * rows * routes.shape[1] // n_sp
    hidden = expert_gate.shape[2]
    if n_sp != 4 or n_tp != 4 or capacity < rows or shared_gate.shape[1] != hidden:
        return shards(*arguments)
    cols = width // n_tp
    heads = queries.shape[1] // HEAD_DIM
    group = queries.shape[1] // keys.shape[1]
    kv_width = keys.shape[1]
    blocks = rows // WINDOW
    bf16, f32 = jnp.bfloat16, jnp.float32
    vmem = pl.BlockSpec(memory_space=pltpu.VMEM)
    anywhere = pl.BlockSpec(memory_space=pl.ANY)
    dma = pltpu.SemaphoreType.DMA
    return pl.pallas_call(
        functools.partial(fused_kernel, (rows, cols, width, WINDOW, hidden, heads, group)),
        out_shape=jax.ShapeDtypeStruct((rows, cols), bf16),
        in_specs=[anywhere]
        + [vmem] * 6
        + [pl.BlockSpec(memory_space=pltpu.SMEM), anywhere, vmem]
        + [anywhere] * 6,
        out_specs=vmem,
        scratch_shapes=[
            pltpu.VMEM((rows, cols), bf16),
            pltpu.VMEM(out_weight.shape, bf16),
            pltpu.VMEM((width, 2 * hidden), bf16),
            pltpu.VMEM((width, 2 * hidden), bf16),
            pltpu.VMEM(expert_down.shape[1:], bf16),
            pltpu.VMEM(shared_down.shape, bf16),
            pltpu.VMEM((WINDOW, kv_width), bf16),
            pltpu.VMEM((WINDOW, kv_width), bf16),
            pltpu.VMEM((8, WINDOW), f32),
            pltpu.VMEM((8, WINDOW), f32),
            pltpu.VMEM((WINDOW, rows), f32),
            pltpu.VMEM((rows, WINDOW), f32),
            pltpu.VMEM((rows, heads * HEAD_DIM), bf16),
            pltpu.VMEM((blocks, 2, WINDOW, cols), bf16),
            pltpu.VMEM((blocks, 2, WINDOW, cols), bf16),
            pltpu.VMEM((blocks, WINDOW, cols), bf16),
            pltpu.VMEM((blocks, WINDOW, cols), bf16),
            pltpu.VMEM((rows, cols), f32),
            pltpu.VMEM((4, 4, rows, cols), bf16),
            pltpu.VMEM((rows, width), bf16),
            pltpu.VMEM((5, 4, rows, hidden), bf16),
            pltpu.VMEM((4, rows, cols), bf16),
            pltpu.VMEM((4, rows, cols), bf16),
            pltpu.VMEM((rows, cols), f32),
            dma((8,)),
            dma((3,)),
            dma((3,)),
            dma((blocks, 3)),
            dma((blocks, 3)),
            dma((7, 4, PARTS)),
            dma((4, 4, PARTS)),
            dma((3, 5, blocks)),
            dma((5, 4, blocks)),
            dma((4, blocks)),
            dma((4, blocks)),
        ],
        compiler_params=pltpu.CompilerParams(collective_id=0, has_side_effects=True),
    )(
        residual,
        queries,
        keys,
        values,
        segments[None, :],
        routes.T,
        route_weight.T,
        sinks,
        out_weight,
        norm_gain[None, :],
        expert_gate,
        expert_up,
        expert_down,
        shared_gate,
        shared_up,
        shared_down,
    )


def solution(mesh):
    placed = (
        P(("grp", "sp"), None),
        P(("grp", "sp"), "tp"),
        P(("grp", "sp"), "tp"),
        P(("grp", "sp"), "tp"),
        P(("grp", "sp")),
        P(("grp", "sp"), None),
        P(("grp", "sp"), None),
        P("tp"),
        P("tp", None),
        P(),
        P("sp", None, "tp"),
        P("sp", None, "tp"),
        P("sp", None, "tp"),
        P(None, "tp"),
        P(None, "tp"),
        P(None, "tp"),
    )
    return jax.shard_map(
        layer, mesh=mesh, in_specs=placed, out_specs=P(("grp", "sp"), "tp"), check_vma=False
    )
```

```python
import functools
import jax
import jax.numpy as jnp
from jax import lax
from jax.experimental import pallas as pl
from jax.experimental.pallas import tpu as pltpu
from jax.sharding import PartitionSpec as P

HEAD_DIM = 64
WINDOW = 128


epsilon = 1e-06


def passed_along(value, axis, steps):
    count = lax.axis_size(axis)
    leading, last = (max(0, -steps), min(count, count - steps))
    return lax.ppermute(value, axis, [(source, source + steps) for source in range(leading, last)])


def banded(prev_rows, own_rows, window_len):
    blocks = own_rows.shape[0] // window_len
    joined = jnp.concatenate([prev_rows, own_rows], axis=0)
    shaped = joined.reshape((blocks + 1, window_len) + own_rows.shape[1:])
    return jnp.concatenate([shaped[:-1], shaped[1:]], axis=1)


def shards(
    residual,
    queries,
    keys,
    values,
    segments,
    routes,
    route_weight,
    sinks,
    out_weight,
    norm_gain,
    expert_gate,
    expert_up,
    expert_down,
    shared_gate,
    shared_up,
    shared_down,
):
    rows_here = residual.shape[0]
    model_width = residual.shape[1]
    tp_count = lax.axis_size("tp")
    tp_index = lax.axis_index("tp")
    head_local = queries.shape[1] // HEAD_DIM
    kv_local = keys.shape[1] // HEAD_DIM
    group_size = head_local // kv_local
    window_len = WINDOW
    blocks = rows_here // window_len
    own_marks = (segments % 256 + 1).astype(jnp.bfloat16)
    prev_keys, prev_values, prev_marks = passed_along(
        (
            keys[rows_here - window_len :],
            values[rows_here - window_len :],
            own_marks[rows_here - window_len :],
        ),
        "sp",
        1,
    )
    key_band = banded(prev_keys, keys, window_len).reshape(
        blocks, 2 * window_len, kv_local, HEAD_DIM
    )
    value_band = banded(prev_values, values, window_len).reshape(
        blocks, 2 * window_len, kv_local, HEAD_DIM
    )
    mark_band = banded(prev_marks, own_marks, window_len).astype(jnp.float32)
    query_marks = own_marks.reshape(blocks, window_len).astype(jnp.float32)
    query_blocks = queries.reshape(blocks, window_len, kv_local, group_size, HEAD_DIM)
    scores = jnp.einsum(
        "nqhgd,nkhd->nhgqk", query_blocks, key_band, preferred_element_type=jnp.float32
    ) * HEAD_DIM ** (-0.5)
    offsets = jnp.arange(window_len)[:, None] + window_len - jnp.arange(2 * window_len)[None, :]
    allowed = (
        (offsets >= 0) & (offsets < window_len) & (query_marks[:, :, None] == mark_band[:, None, :])
    )
    sink_logits = sinks.reshape(kv_local, group_size)[None, :, :, None]
    masked = jnp.where(allowed[:, None, None], scores, -jnp.inf)
    top_score = jnp.maximum(jnp.max(masked, axis=-1), sink_logits)
    exp_terms = jnp.where(allowed[:, None, None], jnp.exp(scores - top_score[..., None]), 0.0)
    denominator = jnp.sum(exp_terms, axis=-1) + jnp.exp(sink_logits - top_score)
    probabilities = (exp_terms / denominator[..., None]).astype(jnp.bfloat16)
    attended = jnp.einsum(
        "nhgqk,nkhd->nqhgd", probabilities, value_band, preferred_element_type=jnp.float32
    )
    attended = attended.astype(jnp.bfloat16).reshape(rows_here, head_local * HEAD_DIM)
    partial_value = jnp.dot(attended, out_weight, preferred_element_type=jnp.float32)
    col_width = model_width // tp_count
    col_start = tp_index * col_width
    summed = lax.psum(partial_value, "tp")
    updated = (residual.astype(jnp.float32) + summed).astype(jnp.bfloat16)
    updated_f32 = updated.astype(jnp.float32)
    inv_rms = lax.rsqrt(jnp.mean(updated_f32 * updated_f32, axis=-1, keepdims=True) + epsilon)
    normed = (updated_f32 * inv_rms * norm_gain).astype(jnp.bfloat16)
    updated_cols = lax.dynamic_slice_in_dim(updated, col_start, col_width, 1)
    normed_cols = lax.dynamic_slice_in_dim(normed, col_start, col_width, 1)
    shared_pre = jnp.dot(normed, shared_gate, preferred_element_type=jnp.float32)
    shared_lin = jnp.dot(normed, shared_up, preferred_element_type=jnp.float32)
    shared_act = (jax.nn.silu(shared_pre) * shared_lin).astype(jnp.bfloat16)
    top_count = routes.shape[1]
    experts = lax.axis_size("sp")
    capacity = 2 * rows_here * top_count // experts
    flat_ids = routes.reshape(-1)
    one_hot = (flat_ids[:, None] == jnp.arange(experts, dtype=jnp.int32)[None, :]).astype(jnp.int32)
    rank_in = jnp.cumsum(one_hot, axis=0) - one_hot
    slot_dest = flat_ids * capacity + jnp.sum(rank_in * one_hot, axis=1)
    token_of = jnp.arange(rows_here * top_count, dtype=jnp.int32) // top_count
    slot_token = jnp.full((experts * capacity,), -1, jnp.int32).at[slot_dest].set(token_of)
    filled = slot_token >= 0
    safe_token = jnp.where(filled, slot_token, 0)
    outgoing = jnp.where(filled[:, None], normed_cols[safe_token], jnp.zeros((), jnp.bfloat16))
    pieces = lax.all_to_all(
        outgoing.reshape(experts, capacity, col_width),
        "sp",
        split_axis=0,
        concat_axis=0,
        tiled=True,
    )
    arrived = lax.all_gather(pieces, "tp", axis=2, tiled=True)
    expert_rows = arrived.reshape(-1, model_width)
    gate_pre = jnp.dot(expert_rows, expert_gate[0], preferred_element_type=jnp.float32)
    up_lin = jnp.dot(expert_rows, expert_up[0], preferred_element_type=jnp.float32)
    expert_act = (jax.nn.silu(gate_pre) * up_lin).astype(jnp.bfloat16)
    gathered_expert, gathered_shared = (
        lax.all_gather(expert_act, "tp", axis=1, tiled=True),
        lax.all_gather(shared_act, "tp", axis=1, tiled=True),
    )
    expert_out = jnp.dot(
        gathered_expert, expert_down[0], preferred_element_type=jnp.float32
    ).astype(jnp.bfloat16)
    returned = lax.all_to_all(
        expert_out.reshape(experts, capacity, col_width),
        "sp",
        split_axis=0,
        concat_axis=0,
        tiled=True,
    )
    returned = returned.reshape(experts * capacity, col_width)
    picked = returned[slot_dest].astype(jnp.float32).reshape(rows_here, top_count, col_width)
    routed = jnp.sum(picked * route_weight[:, :, None], axis=1)
    shared_cols = jnp.dot(gathered_shared, shared_down, preferred_element_type=jnp.float32)
    return (updated_cols.astype(jnp.float32) + shared_cols + routed).astype(jnp.bfloat16)


MESH = pl.DeviceIdType.MESH
PARTS = 4
ALONG = 1


def fused_kernel(
    dims,
    res_hbm,
    q_ref,
    k_ref,
    v_ref,
    seg_ref,
    routes_ref,
    rw_ref,
    sinks_ref,
    wo_hbm,
    gain_ref,
    eg_hbm,
    eu_hbm,
    ed_hbm,
    sg_hbm,
    su_hbm,
    sd_hbm,
    out_ref,
    res_v,
    wo_v,
    gu_v,
    sgu_v,
    dn_v,
    sdn_v,
    kh,
    vh,
    mh,
    marks_v,
    aux_rows,
    aux_ref,
    att,
    b1s,
    b1r,
    b2s,
    b2r,
    keep,
    upd,
    norm_v,
    act,
    eout,
    eback,
    acc,
    w_sem,
    halo_s,
    halo_r,
    b_s,
    b_r,
    u_s,
    u_r,
    a_s,
    a_r,
    e_s,
    e_r,
):
    rows, cols, width, window, hidden, heads, group = dims
    bf16, f32 = jnp.bfloat16, jnp.float32
    s = lax.axis_index("sp")
    t = lax.axis_index("tp")
    core = t % 2
    chip = t // 2
    mate = t + 1 - 2 * core
    over = t + 2 - 4 * chip
    diag = 3 - t

    def remote(src, dst, send, recv, sp, tp):
        return pltpu.make_async_remote_copy(
            src_ref=src,
            dst_ref=dst,
            send_sem=send,
            recv_sem=recv,
            device_id={"sp": sp, "tp": tp},
            device_id_type=MESH,
        )

    barrier = pltpu.get_barrier_semaphore()
    pl.semaphore_signal(barrier, inc=1, device_id={"sp": s, "tp": mate}, device_id_type=MESH)
    pl.semaphore_signal(barrier, inc=1, device_id={"sp": s, "tp": over}, device_id_type=MESH)
    for step in range(1, 4):
        pl.semaphore_signal(
            barrier, inc=1, device_id={"sp": (s + step) % 4, "tp": t}, device_id_type=MESH
        )

    own_cols = pl.ds(pl.multiple_of(t * cols, cols), cols)
    loads = [
        pltpu.make_async_copy(wo_hbm, wo_v, w_sem.at[0]),
        pltpu.make_async_copy(res_hbm.at[:, own_cols], res_v, w_sem.at[1]),
        pltpu.make_async_copy(eg_hbm.at[0], gu_v.at[:, pl.ds(0, hidden)], w_sem.at[2]),
        pltpu.make_async_copy(eu_hbm.at[0], gu_v.at[:, pl.ds(hidden, hidden)], w_sem.at[3]),
        pltpu.make_async_copy(sg_hbm, sgu_v.at[:, pl.ds(0, hidden)], w_sem.at[4]),
        pltpu.make_async_copy(su_hbm, sgu_v.at[:, pl.ds(hidden, hidden)], w_sem.at[5]),
        pltpu.make_async_copy(ed_hbm.at[0], dn_v, w_sem.at[6]),
        pltpu.make_async_copy(sd_hbm, sdn_v, w_sem.at[7]),
    ]
    for load in loads[:2]:
        load.start()

    top_count = routes_ref.shape[0]
    aux_rows[...] = jnp.zeros_like(aux_rows)
    aux_rows[0:1, :] = seg_ref[...].astype(f32)
    aux_rows[1 : 1 + top_count, :] = routes_ref[...].astype(f32)
    aux_rows[1 + top_count : 1 + 2 * top_count, :] = rw_ref[...]
    marks_v[...] = jnp.broadcast_to(aux_rows[0:1, pl.ds(rows - window, window)], (8, window))
    def marks_across(n):
        return aux_rows[0:1, pl.ds(n * window, window)]

    tail = pl.ds(rows - window, window)
    up_sp, down_sp = (s + 1) % 4, (s + 3) % 4
    halos = [
        remote(k_ref.at[tail], kh, halo_s.at[0], halo_r.at[0], up_sp, t),
        remote(v_ref.at[tail], vh, halo_s.at[1], halo_r.at[1], up_sp, t),
        remote(marks_v, mh, halo_s.at[2], halo_r.at[2], up_sp, t),
    ]

    @pl.when(s == 0)
    def _():
        kh[...] = jnp.zeros_like(kh)
        vh[...] = jnp.zeros_like(vh)
        mh[...] = jnp.full(mh.shape, -1.0, f32)

    for n in range(rows // window):
        here = pl.ds(n * window, window)
        aux_ref[here, :] = jnp.transpose(aux_rows[:, here])

    q_pos = lax.broadcasted_iota(jnp.int32, (window, window), 0)
    k_pos = lax.broadcasted_iota(jnp.int32, (window, window), 1)

    def attend(n):
        here = pl.ds(n * window, window)
        if n == 0:
            k_prev, v_prev, m_prev = kh[...], vh[...], mh[0:1, :]
        else:
            before = pl.ds((n - 1) * window, window)
            k_prev, v_prev, m_prev = k_ref[before, :], v_ref[before, :], marks_across(n - 1)
        k_own, v_own, m_own = k_ref[here, :], v_ref[here, :], marks_across(n)
        marks = aux_ref[here, 0:1]
        ok_prev = (k_pos > q_pos) & (marks == m_prev)
        ok_own = (k_pos <= q_pos) & (marks == m_own)
        for h in range(heads):
            kv = slice((h // group) * HEAD_DIM, (h // group + 1) * HEAD_DIM)
            qh = q_ref[here, h * HEAD_DIM : (h + 1) * HEAD_DIM]
            contract = (((1,), (1,)), ((), ()))
            sc_prev = lax.dot_general(
                qh, k_prev[:, kv], contract, preferred_element_type=f32
            ) * HEAD_DIM ** (-0.5)
            sc_own = lax.dot_general(
                qh, k_own[:, kv], contract, preferred_element_type=f32
            ) * HEAD_DIM ** (-0.5)
            sc_prev = jnp.where(ok_prev, sc_prev, -jnp.inf)
            sc_own = jnp.where(ok_own, sc_own, -jnp.inf)
            sink = sinks_ref[h]
            top = jnp.maximum(
                jnp.max(jnp.maximum(sc_prev, sc_own), axis=-1, keepdims=True), sink
            )
            ex_prev = jnp.exp(sc_prev - top)
            ex_own = jnp.exp(sc_own - top)
            total = jnp.sum(ex_prev + ex_own, axis=-1, keepdims=True) + jnp.exp(sink - top)
            inverse = 1.0 / total
            p_prev = (ex_prev * inverse).astype(bf16)
            p_own = (ex_own * inverse).astype(bf16)
            got = jnp.dot(p_prev, v_prev[:, kv], preferred_element_type=f32) + jnp.dot(
                p_own, v_own[:, kv], preferred_element_type=f32
            )
            att[here, h * HEAD_DIM : (h + 1) * HEAD_DIM] = got.astype(bf16)

    def project(n, chunk):
        where = pl.ds(pl.multiple_of(chunk * cols, cols), cols)
        return jnp.dot(
            att[pl.ds(n * window, window), :], wo_v[:, where], preferred_element_type=f32
        )

    halves = list(range(rows // window))[::-1]
    attend(halves[0])
    pl.semaphore_wait(barrier, 5)

    @pl.when(s < 3)
    def _():
        for copy in halos:
            copy.start()

    pending = []
    first = {}
    second = {}
    for n in halves:
        if n == 0:

            @pl.when(s > 0)
            def _():
                for copy in halos:
                    copy.wait_recv()

        if n != halves[0]:
            attend(n)
        else:
            loads[0].wait()
            for load in loads[2:]:
                load.start()
        for far in (1, 0):
            chunk = (over if far else t) + 1 - 2 * core
            b1s[n, far] = project(n, chunk).astype(bf16)
            copy = remote(
                b1s.at[n, far], b1r.at[n, far], b_s.at[n, far], b_r.at[n, far], s, mate
            )
            copy.start()
            pending.append(copy)
            first[n, far] = copy
        mine = project(n, over)
        first[n, 1].wait_recv()
        b2s[n] = (mine + b1r[n, 1].astype(f32)).astype(bf16)
        copy = remote(b2s.at[n], b2r.at[n], b_s.at[n, 2], b_r.at[n, 2], s, over)
        copy.start()
        pending.append(copy)
        second[n] = copy
    loads[1].wait()
    for n in halves:
        here = pl.ds(n * window, window)
        mine = project(n, t) + res_v[here, :].astype(f32)
        first[n, 0].wait_recv()
        keep[here, :] = mine + b1r[n, 0].astype(f32)

    parts = u_s.shape[2]
    part_rows = rows // parts
    per_half = window // part_rows
    listed = [n * per_half + i for n in halves for i in range(per_half)]

    def of_half(n):
        return [p for p in listed if n is None or p // per_half == n]

    def piece(b, chunk, n):
        return upd.at[b, chunk, pl.ds(n * part_rows, part_rows)]

    def share(kind, k, b, chunk, n, sp, tp):
        return remote(
            piece(b, chunk, n),
            piece(b, chunk, n),
            u_s.at[kind, k, n],
            u_r.at[b, chunk, n],
            sp,
            tp,
        )

    conditional = []
    for n in halves:
        here = pl.ds(n * window, window)
        second[n].wait_recv()
        upd[s, t, here, :] = (keep[here, :] + b2r[n].astype(f32)).astype(bf16)
        for p in of_half(n):
            over_copy = share(3, 0, s, t, p, s, over)
            over_copy.start()
            up_copy = share(0, 0, s, t, p, up_sp, t)
            down_copy = share(1, 0, s, t, p, down_sp, t)

            @pl.when(s < 3)
            def _(up_copy=up_copy):
                up_copy.start()

            @pl.when(s > 0)
            def _(down_copy=down_copy):
                down_copy.start()

            mate_copy = share(2, 0, s, t, p, s, mate)
            mate_copy.start()
            pending += [over_copy, mate_copy]
            conditional += [(s < 3, up_copy), (s > 0, down_copy)]

    side = s // 2
    edge = s + side * (3 - 2 * s)
    order = [s]
    for k in range(1, 4):
        flat = (k, k + edge, k - 2 * edge, k)[k]
        order.append(flat + side * (3 - 2 * flat))

    along = listed[:ALONG]

    def onward(k, kinds, chunk, n):
        b = order[k]
        to_up = share(kinds[0], k, b, chunk, n, up_sp, t)
        to_down = share(kinds[1], k, b, chunk, n, down_sp, t)
        rising = s < 3 if k == 0 else (b < s) & (s < 3)
        falling = s > 0 if k == 0 else (b > s) & (s > 0)

        @pl.when(rising)
        def _():
            to_up.start()

        @pl.when(falling)
        def _():
            to_down.start()

        conditional.extend([(rising, to_up), (falling, to_down)])

    def arrive(k, half=None):
        b = order[k]
        for n in of_half(half):
            share(0, k, b, t, n, s, mate).wait_recv()
            onward(k, (0, 1), t, n)
            if n not in along:
                copy = share(3, k, b, t, n, s, over)
                copy.start()
                pending.append(copy)
            mate_copy = share(2, k, b, t, n, s, mate)
            mate_copy.start()
            pending.append(mate_copy)

    def relay_half(k, n):
        b = order[k]
        share(4, k, b, over, n, s, mate).wait_recv()
        if n in along:
            onward(k, (5, 6), over, n)
        copy = share(4, k, b, over, n, s, mate)
        copy.start()
        pending.append(copy)

    def relay(k, half=None):
        for n in of_half(half):
            if k == 0 or n not in along:
                relay_half(k, n)

    def arrive_over(k):
        for n in along:
            relay_half(k, n)

    def span_of(half):
        if half is None:
            return halves, 0, rows
        return [half], half * window, window

    def normalize(k, half=None):
        b = order[k]
        _, begin, length = span_of(half)
        for n in of_half(half):
            share(2, k, b, mate, n, s, mate).wait_recv()
            share(4, k, b, diag, n, s, mate).wait_recv()
        step = 32

        def body(i, carry):
            here = pl.ds(pl.multiple_of(begin + i * step, step), step)
            squares = jnp.zeros((step, 1), f32)
            for chunk in range(4):
                part = upd[b, chunk, here, :].astype(f32)
                squares = squares + jnp.sum(part * part, axis=-1, keepdims=True)
            inv = lax.rsqrt(squares / width + epsilon)
            for chunk in range(4):
                part = upd[b, chunk, here, :].astype(f32)
                span = slice(chunk * cols, (chunk + 1) * cols)
                norm_v[here, span] = (part * inv * gain_ref[0:1, span]).astype(bf16)
            return carry

        lax.fori_loop(0, length // step, body, 0)

    def pass_on(slot, kind, chunk, tp, half):
        place = act.at[slot, chunk, pl.ds(half * window, window)]
        return remote(
            place, place, a_s.at[kind, slot, half], a_r.at[slot, chunk, half], s, tp
        )

    def activate(slot, weight, half=None):
        _, begin, length = span_of(half)
        here = pl.ds(begin, length)
        both = jnp.dot(norm_v[here, :], weight[...], preferred_element_type=f32)
        gate, lin = both[:, :hidden], both[:, hidden:]
        act[slot, t, here, :] = (gate / (1.0 + jnp.exp(-gate)) * lin).astype(bf16)

    def ship(slot, half=None):
        for n in span_of(half)[0]:
            for kind, tp in ((0, over), (1, mate)):
                copy = pass_on(slot, kind, t, tp, n)
                copy.start()
                pending.append(copy)

    def relay_act(slot, half=None):
        for n in span_of(half)[0]:
            pass_on(slot, 2, over, mate, n).wait_recv()
            copy = pass_on(slot, 2, over, mate, n)
            copy.start()
            pending.append(copy)

    def contract_act(slot, weight, half=None):
        listing, begin, length = span_of(half)
        for n in listing:
            pass_on(slot, 1, mate, mate, n).wait_recv()
            pass_on(slot, 2, diag, mate, n).wait_recv()
        total = None
        for chunk in range(4):
            part = jnp.dot(
                act[slot, chunk, pl.ds(begin, length), :],
                weight[chunk * hidden : (chunk + 1) * hidden, :],
                preferred_element_type=f32,
            )
            total = part if total is None else total + part
        return total

    def give_back(k, b, half):
        here = pl.ds(half * window, window)
        return remote(
            eout.at[k, here], eback.at[b, here], e_s.at[k, half], e_r.at[b, half], order[k], t
        )

    def finish(k, half=None):
        listing, begin, length = span_of(half)
        eout[k, pl.ds(begin, length), :] = contract_act(k, dn_v, half).astype(bf16)
        for n in listing:
            copy = give_back(k, s, n)
            copy.start()
            pending.append(copy)

    def expert(k, half=None):
        normalize(k, half)
        activate(k, gu_v, half)
        ship(k, half)

    early, late = halves[0], halves[-1]
    arrive(1)
    relay(0)
    arrive(2)
    arrive_over(1)
    relay(1)
    loads[2].wait()
    loads[3].wait()
    expert(1)
    arrive(3, early)
    arrive_over(2)
    normalize(0)
    activate(0, gu_v)
    relay(2)
    loads[4].wait()
    loads[5].wait()
    activate(4, sgu_v)
    expert(2)
    relay_act(1)
    loads[6].wait()
    finish(1)
    arrive(3, late)
    arrive_over(3)
    relay(3, early)
    expert(3, early)
    relay_act(2)
    finish(2)
    relay(3, late)
    expert(3, late)
    ship(0)
    ship(4)
    relay_act(3, early)
    finish(3, early)
    relay_act(3, late)
    finish(3, late)
    relay_act(0)
    relay_act(4)
    eout[0] = contract_act(0, dn_v).astype(bf16)
    loads[7].wait()
    acc[...] = contract_act(4, sdn_v)

    def weight_of(e):
        total = jnp.zeros((rows, 1), f32)
        for k in range(1, top_count + 1):
            weight = aux_ref[:, top_count + k : top_count + k + 1]
            named = aux_ref[:, k : k + 1] == jnp.full((rows, 1), e, jnp.int32).astype(f32)
            total = total + jnp.where(named, weight, 0.0)
        return total

    weights = [weight_of(order[k]) for k in range(4)]
    for n in halves:
        here = pl.ds(n * window, window)
        acc[here, :] = (
            acc[here, :]
            + upd[s, t, here, :].astype(f32)
            + weights[0][n * window : (n + 1) * window] * eout[0, here, :].astype(f32)
        )
    for k in range(1, 4):
        for n in halves:
            here = pl.ds(n * window, window)
            give_back(k, order[k], n).wait_recv()
            more = weights[k][n * window : (n + 1) * window] * eback[order[k], here, :].astype(f32)
            if k < 3:
                acc[here, :] = acc[here, :] + more
            else:
                out_ref[here, :] = (acc[here, :] + more).astype(bf16)

    for copy in pending:
        copy.wait_send()
    for when, copy in conditional:

        @pl.when(when)
        def _():
            copy.wait_send()

    @pl.when(s < 3)
    def _():
        for copy in halos:
            copy.wait_send()


def layer(
    residual,
    queries,
    keys,
    values,
    segments,
    routes,
    route_weight,
    sinks,
    out_weight,
    norm_gain,
    expert_gate,
    expert_up,
    expert_down,
    shared_gate,
    shared_up,
    shared_down,
):
    arguments = (
        residual,
        queries,
        keys,
        values,
        segments,
        routes,
        route_weight,
        sinks,
        out_weight,
        norm_gain,
        expert_gate,
        expert_up,
        expert_down,
        shared_gate,
        shared_up,
        shared_down,
    )
    rows, width = residual.shape
    n_sp, n_tp = lax.axis_size("sp"), lax.axis_size("tp")
    capacity = 2 * rows * routes.shape[1] // n_sp
    hidden = expert_gate.shape[2]
    if n_sp != 4 or n_tp != 4 or capacity < rows or rows < 2 * WINDOW or shared_gate.shape[1] != hidden:
        return shards(*arguments)
    cols = width // n_tp
    heads = queries.shape[1] // HEAD_DIM
    group = queries.shape[1] // keys.shape[1]
    kv_width = keys.shape[1]
    blocks = rows // WINDOW
    bf16, f32 = jnp.bfloat16, jnp.float32
    vmem = pl.BlockSpec(memory_space=pltpu.VMEM)
    anywhere = pl.BlockSpec(memory_space=pl.ANY)
    dma = pltpu.SemaphoreType.DMA
    return pl.pallas_call(
        functools.partial(fused_kernel, (rows, cols, width, WINDOW, hidden, heads, group)),
        out_shape=jax.ShapeDtypeStruct((rows, cols), bf16),
        in_specs=[anywhere]
        + [vmem] * 6
        + [pl.BlockSpec(memory_space=pltpu.SMEM), anywhere, vmem]
        + [anywhere] * 6,
        out_specs=vmem,
        scratch_shapes=[
            pltpu.VMEM((rows, cols), bf16),
            pltpu.VMEM(out_weight.shape, bf16),
            pltpu.VMEM((width, 2 * hidden), bf16),
            pltpu.VMEM((width, 2 * hidden), bf16),
            pltpu.VMEM(expert_down.shape[1:], bf16),
            pltpu.VMEM(shared_down.shape, bf16),
            pltpu.VMEM((WINDOW, kv_width), bf16),
            pltpu.VMEM((WINDOW, kv_width), bf16),
            pltpu.VMEM((8, WINDOW), f32),
            pltpu.VMEM((8, WINDOW), f32),
            pltpu.VMEM((WINDOW, rows), f32),
            pltpu.VMEM((rows, WINDOW), f32),
            pltpu.VMEM((rows, heads * HEAD_DIM), bf16),
            pltpu.VMEM((blocks, 2, WINDOW, cols), bf16),
            pltpu.VMEM((blocks, 2, WINDOW, cols), bf16),
            pltpu.VMEM((blocks, WINDOW, cols), bf16),
            pltpu.VMEM((blocks, WINDOW, cols), bf16),
            pltpu.VMEM((rows, cols), f32),
            pltpu.VMEM((4, 4, rows, cols), bf16),
            pltpu.VMEM((rows, width), bf16),
            pltpu.VMEM((5, 4, rows, hidden), bf16),
            pltpu.VMEM((4, rows, cols), bf16),
            pltpu.VMEM((4, rows, cols), bf16),
            pltpu.VMEM((rows, cols), f32),
            dma((8,)),
            dma((3,)),
            dma((3,)),
            dma((blocks, 3)),
            dma((blocks, 3)),
            dma((7, 4, PARTS)),
            dma((4, 4, PARTS)),
            dma((3, 5, blocks)),
            dma((5, 4, blocks)),
            dma((4, blocks)),
            dma((4, blocks)),
        ],
        compiler_params=pltpu.CompilerParams(collective_id=0, has_side_effects=True),
    )(
        residual,
        queries,
        keys,
        values,
        segments[None, :],
        routes.T,
        route_weight.T,
        sinks,
        out_weight,
        norm_gain[None, :],
        expert_gate,
        expert_up,
        expert_down,
        shared_gate,
        shared_up,
        shared_down,
    )


def solution(mesh):
    placed = (
        P(("grp", "sp"), None),
        P(("grp", "sp"), "tp"),
        P(("grp", "sp"), "tp"),
        P(("grp", "sp"), "tp"),
        P(("grp", "sp")),
        P(("grp", "sp"), None),
        P(("grp", "sp"), None),
        P("tp"),
        P("tp", None),
        P(),
        P("sp", None, "tp"),
        P("sp", None, "tp"),
        P("sp", None, "tp"),
        P(None, "tp"),
        P(None, "tp"),
        P(None, "tp"),
    )
    return jax.shard_map(
        layer, mesh=mesh, in_specs=placed, out_specs=P(("grp", "sp"), "tp"), check_vma=False
    )
```
